512 devices in a mesh: sp: 32 (over z, core), tp: 16 (over y, x).
Axes of the slice: x: 4, y: 4, z: 16, core: 2. Of those that a mesh axis runs over, the one named last changes fastest.
Arguments:
- moe_input: bfloat16 [8192, 2048], P('sp'), may hold values from -6 to 6
- out_grad: bfloat16 [8192, 2048], P('sp'), may hold values from -0.29882812 to 0.29882812
- route_ids: int32 [8192, 2], P('sp'), may hold values from 0 to 31, all different within a row; in each aligned block of 256 rows (0 to 255, 256 to 511, ...) at most 20 rows name the same one
- route_weights: float32 [8192, 2], P('sp'), may hold values from 0.2 to 1
- gate_weight: bfloat16 [32, 1024, 2048], P('sp', 'tp'), may hold values from -0.1875 to 0.1875
- lin_weight: bfloat16 [32, 1024, 2048], P('sp', 'tp'), may hold values from -0.1875 to 0.1875
- down_weight: bfloat16 [32, 1024, 2048], P('sp', 'tp'), may hold values from -0.1875 to 0.1875
- outer_gate: bfloat16 [8192, 2048], P('sp', 'tp'), may hold values from -6 to 6
- inner_gate: bfloat16 [8192, 2048], P('sp', 'tp'), may hold values from -6 to 6
- conv_input: bfloat16 [8192, 2048], P('sp', 'tp'), may hold values from -6 to 6
- conv_taps: float32 [3, 2048], P(None, 'tp'), may hold values from -3.5 to 3.5
- out_proj: bfloat16 [2048, 2048], P('tp', 'sp'), may hold values from -0.125 to 0.125
Outputs:
- gate_weight_grad: bfloat16 [32, 1024, 2048], P('sp', 'tp')
- lin_weight_grad: bfloat16 [32, 1024, 2048], P('sp', 'tp')
- down_weight_grad: bfloat16 [32, 1024, 2048], P('sp', 'tp')
- out_proj_grad: float32 [2048, 2048], P('sp', 'tp')
- outer_gate_grad: bfloat16 [8192, 2048], P('sp', 'tp')
- inner_gate_grad: bfloat16 [8192, 2048], P('sp', 'tp')
- conv_input_grad: bfloat16 [8192, 2048], P('sp', 'tp')
The draws below stay inside these ranges and needn't reach their ends.
Inputs may be any that keep to these rules, and one draw needn't show every extreme that they name: `route_ids`: each row names 2 different experts. Among the rows of one device no expert is named more than 20 times, a bound that some block reaches.
All inputs are finite; a program needn't handle non-finite values.
Results may differ from the reference program's by a relative error of at most 0.015.
Values may be sent and summed in bfloat16 or wider, within the bound.
No kernel may reach another device: no remote copies, remote signals or barrier semaphores. Data moves between devices by JAX's collectives and lax.ppermute only.
A program may use at most 64 MiB of HBM per device.

```python
import math
from functools import partial
import jax
import jax.numpy as jnp
import numpy as np
from jax import lax

D = 2048
FF = 1024
TOP = 2
TAPS = 3
TOK_DEV = 256
TOKENS = 8192
EXPERTS = 32
CAP = 20
FF_DEV = 64
N_SP = 32
N_TP = 16


def with_spikes(result, own_key, source, target, parts, factor):
    def block_of(dim):
        return (jnp.arange(result.shape[dim]) // (result.shape[dim] // parts)).reshape((-1,) + (1,) * (result.ndim - 1 - dim))

    first = jax.random.permutation(own_key, parts)[block_of(target)]
    other_side = (block_of(target) + parts // 2) % parts
    return jnp.where((block_of(source) == first) | (block_of(source) == other_side), factor * result, result)


def steps_of(own_key, dims, split, low, high):
    factor_of, own = 1.0, jax.random.fold_in(own_key, 6)
    for axis_at, shards_of in split:
        heights = jnp.exp(jax.random.uniform(jax.random.fold_in(own, axis_at), (shards_of,), jnp.float32, low / len(split), high / len(split)))
        factor_of = factor_of * jnp.repeat(heights, dims[axis_at] // shards_of).reshape([-1 if axis == axis_at else 1 for axis in range(len(dims))])
    return factor_of


def shared_out(rng, own, number, rows, number_of, top, limit, skew):
    sequence = jax.random.permutation(rng, number_of)
    packed, common = load_shares(number_of, rows * top, limit, skew, True), load_shares(number_of, rows * top, limit, skew, False)
    places = jnp.arange(number_of)

    def named(lengths, offset_by):
        used = int((lengths > 0).sum())
        fixed = max(1, used // 4)
        moved = fixed + (places - fixed + offset_by * (used - fixed)) % max(1, number_of - fixed)
        return jnp.zeros((number_of,), jnp.int32).at[sequence[jnp.where(places < fixed, places, moved)]].set(jnp.asarray(lengths, jnp.int32))

    lengths = jnp.where(number % 4 == 0, named(packed, number // 4), named(common, number - number // 4 - 1))
    mixed = jax.random.permutation(jax.random.fold_in(own, 3), number_of)
    source_of, receiver = mixed[0:number_of // 2 * 2:2], mixed[1:number_of // 2 * 2:2]
    margin = jnp.minimum(lengths[source_of] - 1, limit - lengths[receiver]) // 2
    margin = jnp.where((source_of == sequence[0]) | (receiver == sequence[0]) | (lengths[receiver] == 0), 0, jnp.maximum(margin, 0))
    moved = jax.random.randint(jax.random.fold_in(own, 4), (number_of // 2,), 0, 1 << 20) % (margin + 1)
    lengths = lengths.at[source_of].add(-moved).at[receiver].add(moved)
    items = jnp.searchsorted(jnp.cumsum(lengths), jnp.arange(rows * top), side="right").astype(jnp.int32)
    grid = items.reshape(top, rows).T
    grid = grid[jax.random.permutation(jax.random.fold_in(own, 1), rows)]
    offset_by = jax.random.randint(jax.random.fold_in(own, 2), (rows, 1), 0, top)
    return jnp.take_along_axis(grid, (jnp.arange(top)[None, :] + offset_by) % top, axis=1)


def load_shares(count, total, limit, skew, full):
    weights = [(1 << 20) // math.isqrt(rank ** skew) + 1 for rank in range(1, count + 1)]
    largest = limit if full else min(limit, max(-(-total // count), total * weights[0] // sum(weights)))
    least = 1 if total - largest >= count - 1 else 0
    given, rest = [largest] + [least] * (count - 1), total - largest - least * (count - 1)
    while rest > 0:
        free = [i for i in range(1, count) if given[i] < largest] or [i for i in range(1, count) if given[i] < limit]
        mass, left = sum([weights[i] for i in free]), rest
        for i in free:
            addition = min(limit - given[i], max(1, left * weights[i] // mass), rest)
            given[i] = given[i] + addition
            rest = rest - addition
    return np.array(given)


def noise(stream_key, shape, width, reach, shards=(), kind=jnp.bfloat16):
    gain = steps_of(stream_key, shape, shards, -0.22, 0.18) if shards else 1.0
    drawn = jax.random.normal(stream_key, shape, jnp.float32) * width * gain
    return jnp.minimum(jnp.maximum(drawn, -reach), reach).astype(kind)


def heavy_noise(key, dims, deviation, bound, shards, heavy, held_as=jnp.bfloat16):
    drawn = deviation * jax.random.normal(key, dims, jnp.float32)
    if shards:
        drawn = drawn * steps_of(key, dims, shards, -0.22, 0.18)
    return jnp.clip(with_spikes(drawn, jax.random.fold_in(key, 3), *heavy), -bound, bound).astype(held_as)


def setup_inputs(seed: int = 0) -> dict:
    keys = jax.random.split(jax.random.key(seed), 13)
    moe_input = noise(keys[0], (TOKENS, D), 1.0, 6.0, ((0, 32),))
    out_grad = heavy_noise(keys[1], (TOKENS, D), 0.05, 0.29882812, ((0, 32),), (0, 1, 32, 2.75))
    route_ids_keys = jax.random.split(jax.random.fold_in(keys[2], 1), TOKENS // TOK_DEV)
    route_ids_turns = jax.random.permutation(jax.random.fold_in(keys[2], 3), TOKENS // TOK_DEV)
    route_ids = jax.vmap(lambda own, number: shared_out(jax.random.fold_in(keys[2], 2), own, number, TOK_DEV, EXPERTS, TOP, CAP, 1))(route_ids_keys, route_ids_turns).reshape((TOKENS, TOP))
    route_weights = jnp.clip(0.2 + 0.8 * jax.random.uniform(keys[3], (TOKENS, TOP), jnp.float32) ** steps_of(keys[3], (TOKENS, TOP), ((0, 32),), -0.2, 0.2), 0.2, 1.0)
    gate_weight = noise(keys[4], (EXPERTS, FF, D), (D // 2) ** -0.5, 0.1875, ((0, 32), (1, 16)))
    lin_weight = noise(keys[5], (EXPERTS, FF, D), (D // 2) ** -0.5, 0.1875, ((0, 32), (1, 16)))
    down_weight = noise(keys[6], (EXPERTS, FF, D), FF ** -0.5, 0.1875, ((0, 32), (1, 16)))
    outer_gate = noise(keys[7], (TOKENS, D), 1.0, 6.0, ((0, 32), (1, 16)))
    inner_gate = noise(keys[8], (TOKENS, D), 1.0, 6.0, ((0, 32), (1, 16)))
    conv_input = noise(keys[9], (TOKENS, D), 1.0, 6.0, ((0, 32), (1, 16)))
    conv_taps = noise(keys[10], (TAPS, D), 3 ** -0.5, 3.5, ((1, 16),), jnp.float32)
    out_proj = noise(keys[11], (D, D), D ** -0.5, 0.125, ((0, 16), (1, 32)))
    return dict(moe_input=moe_input, out_grad=out_grad, route_ids=route_ids, route_weights=route_weights, gate_weight=gate_weight, lin_weight=lin_weight, down_weight=down_weight, outer_gate=outer_gate, inner_gate=inner_gate, conv_input=conv_input, conv_taps=conv_taps, out_proj=out_proj)


LIMIT = 7.0
ALPHA = 1.702


def slot_layout(flat_ids, experts, capacity):
    onehot = (flat_ids[:, None] == jnp.arange(experts, dtype=jnp.int32)[None, :]).astype(jnp.int32)
    before = (jnp.cumsum(onehot, axis=0) - onehot).astype(jnp.int32)
    slot_rank = jnp.sum(before * onehot, axis=1).astype(jnp.int32)
    position = (flat_ids.astype(jnp.int32) * capacity + slot_rank).astype(jnp.int32)
    pair_index = jnp.arange(flat_ids.shape[0], dtype=jnp.int32)
    source = jnp.full((experts * capacity,), -1, jnp.int32).at[position].set(pair_index)
    return position, source


def one_expert(operands):
    routed, cotan, gate_w, lin_w, down_w = operands
    routed = routed.astype(jnp.float32)
    cotan = cotan.astype(jnp.float32)
    gate_f = gate_w.astype(jnp.float32)
    lin_f = lin_w.astype(jnp.float32)
    gate_pre = jnp.dot(gate_f, routed.T)
    lin_pre = jnp.dot(lin_f, routed.T)
    gate_cut = jnp.minimum(gate_pre, LIMIT)
    lin_cut = jnp.clip(lin_pre, -LIMIT, LIMIT)
    sigma = jax.nn.sigmoid(ALPHA * gate_cut)
    act = (gate_cut * sigma * (lin_cut + 1.0)).astype(jnp.bfloat16)
    act_grad = jnp.dot(down_w.astype(jnp.float32), cotan.T)
    down_grad = jnp.dot(act.astype(jnp.float32), cotan).astype(jnp.bfloat16)
    slope = sigma * (1.0 + ALPHA * gate_cut * (1.0 - sigma))
    gate_cot = jnp.where(gate_pre < LIMIT, act_grad * (lin_cut + 1.0) * slope, 0.0).astype(jnp.bfloat16)
    lin_cot = jnp.where(jnp.abs(lin_pre) < LIMIT, act_grad * gate_cut * sigma, 0.0).astype(jnp.bfloat16)
    gate_grad = jnp.dot(gate_cot.astype(jnp.float32), routed).astype(jnp.bfloat16)
    lin_grad = jnp.dot(lin_cot.astype(jnp.float32), routed).astype(jnp.bfloat16)
    slots = routed.shape[0]
    gate_blocks = gate_cot.astype(jnp.float32).reshape(N_TP, FF_DEV, slots)
    lin_blocks = lin_cot.astype(jnp.float32).reshape(N_TP, FF_DEV, slots)
    partial_sums = jnp.einsum("bfr,bfd->brd", gate_blocks, gate_f.reshape(N_TP, FF_DEV, D))
    partial_sums = partial_sums + jnp.einsum("bfr,bfd->brd", lin_blocks, lin_f.reshape(N_TP, FF_DEV, D))
    partial_sums = partial_sums.astype(jnp.bfloat16).astype(jnp.float32)
    slot_grads = jnp.sum(partial_sums, axis=0).astype(jnp.bfloat16)
    return gate_grad, lin_grad, down_grad, slot_grads


def reference(moe_input, out_grad, route_ids, route_weights, gate_weight, lin_weight, down_weight, outer_gate, inner_gate, conv_input, conv_taps, out_proj):
    block_ids = route_ids.reshape(N_SP, TOK_DEV * TOP)
    position, source = jax.vmap(partial(slot_layout, experts=EXPERTS, capacity=CAP))(block_ids)
    source = source.reshape(N_SP, EXPERTS, CAP).transpose(1, 0, 2)
    block_base = (jnp.arange(N_SP, dtype=jnp.int32) * (TOK_DEV * TOP)).astype(jnp.int32)
    filled = source >= 0
    global_pair = jnp.where(filled, source + block_base[None, :, None], 0).astype(jnp.int32)
    filled = filled.reshape(EXPERTS, N_SP * CAP)
    global_pair = global_pair.reshape(EXPERTS, N_SP * CAP)
    token_row = (global_pair // TOP).astype(jnp.int32)
    routed_rows = jnp.where(filled[:, :, None], moe_input[token_row], jnp.zeros((), jnp.bfloat16))
    slot_weight = jnp.where(filled, route_weights.reshape(-1)[global_pair], 0.0)
    routed_grads = (slot_weight[:, :, None] * out_grad[token_row].astype(jnp.float32)).astype(jnp.bfloat16)
    gate_weight_grad, lin_weight_grad, down_weight_grad, slot_grads = lax.map(
        one_expert, (routed_rows, routed_grads, gate_weight, lin_weight, down_weight))
    slot_grads = slot_grads.reshape(EXPERTS, N_SP, CAP, D).transpose(1, 0, 2, 3).reshape(N_SP, EXPERTS * CAP, D)
    pair_grads = jax.vmap(lambda table, where_at: table[where_at])(slot_grads, position)
    row_grads = jnp.sum(pair_grads.astype(jnp.float32).reshape(TOKENS, TOP, D), axis=1).astype(jnp.bfloat16)
    stream_grad = (out_grad.astype(jnp.float32) + row_grads.astype(jnp.float32)).astype(jnp.bfloat16)
    conv_values = (inner_gate.astype(jnp.float32) * conv_input.astype(jnp.float32)).astype(jnp.bfloat16)
    padded = jnp.pad(conv_values.astype(jnp.float32), ((TAPS - 1, 0), (0, 0)))
    convolved = jnp.zeros((TOKENS, D), jnp.float32)
    for tap_index in range(TAPS):
        convolved = convolved + conv_taps[tap_index][None, :] * padded[tap_index:tap_index + TOKENS]
    mixed = (outer_gate.astype(jnp.float32) * convolved).astype(jnp.bfloat16)
    mixed_grad = jnp.dot(stream_grad, out_proj.T, preferred_element_type=jnp.float32)
    out_proj_grad = jnp.dot(stream_grad.T, mixed, preferred_element_type=jnp.float32)
    outer_gate_grad = (mixed_grad * convolved).astype(jnp.bfloat16)
    conv_cot = (mixed_grad * outer_gate.astype(jnp.float32)).astype(jnp.bfloat16)
    padded_cot = jnp.pad(conv_cot.astype(jnp.float32), ((0, TAPS - 1), (0, 0)))
    value_grad = jnp.zeros((TOKENS, D), jnp.float32)
    for tap_index in range(TAPS):
        first_row = TAPS - 1 - tap_index
        value_grad = value_grad + conv_taps[tap_index][None, :] * padded_cot[first_row:first_row + TOKENS]
    inner_gate_grad = (value_grad * conv_input.astype(jnp.float32)).astype(jnp.bfloat16)
    conv_input_grad = (value_grad * inner_gate.astype(jnp.float32)).astype(jnp.bfloat16)
    return (gate_weight_grad, lin_weight_grad, down_weight_grad, out_proj_grad, outer_gate_grad, inner_gate_grad, conv_input_grad)
```

```python
import jax
import jax.numpy as jnp
from jax import lax
from jax.sharding import Mesh
from jax.sharding import PartitionSpec as P

SP = ("z", "c")
TP = ("y", "x")
LIMIT = 7.0
ALPHA = 1.702
BF = jnp.bfloat16
F32 = jnp.float32


def swap(blocks, axis):
    return lax.all_to_all(blocks, axis, split_axis=0, concat_axis=0, tiled=True)


def from_everyone(value, axis):
    return swap(jnp.broadcast_to(value, (lax.axis_size(axis), *value.shape)), axis)


def turned(value, axis, by):
    count = lax.axis_size(axis)
    return lax.ppermute(value, axis, [(i, (i + by) % count) for i in range(count)])


def mirrored(value, axis, bit):
    return lax.ppermute(value, axis, [(i, i ^ bit) for i in range(lax.axis_size(axis))])


def doubled(value, axis):
    index = lax.axis_index(axis)
    bit = lax.axis_size(axis) // 2
    while bit:
        other = mirrored(value, axis, bit)
        high = (index & bit) > 0
        both = (jnp.where(high, other, value), jnp.where(high, value, other))
        value = jnp.stack(both, axis=value.ndim - 2)
        bit //= 2
    return value


def from_behind(value, axis, by):
    count = lax.axis_size(axis)
    pairs = [(i, i + by) for i in range(count) if 0 <= i + by < count]
    return lax.ppermute(value, axis, pairs)


def dot(a, b, ca, cb):
    return lax.dot_general(a, b, (((ca,), (cb,)), ((), ())), preferred_element_type=F32)


def expert_cots(rows, grads, gate_w, lin_w, down_w):
    gate_pre = dot(rows, gate_w, 1, 1)
    lin_pre = dot(rows, lin_w, 1, 1)
    act_grad = dot(grads, down_w, 1, 1)
    gate_cut = jnp.minimum(gate_pre, LIMIT)
    lin_cut = jnp.clip(lin_pre, -LIMIT, LIMIT)
    sigma = jax.nn.sigmoid(ALPHA * gate_cut)
    act = (gate_cut * sigma * (lin_cut + 1.0)).astype(BF)
    slope = sigma * (1.0 + ALPHA * gate_cut * (1.0 - sigma))
    gate_cot = jnp.where(gate_pre < LIMIT, act_grad * (lin_cut + 1.0) * slope, 0.0).astype(BF)
    lin_cot = jnp.where(jnp.abs(lin_pre) < LIMIT, act_grad * gate_cut * sigma, 0.0).astype(BF)
    return act, gate_cot, lin_cot


def local(
    moe_input,
    out_grad,
    route_ids,
    route_weights,
    gate_weight,
    lin_weight,
    down_weight,
    outer_gate,
    inner_gate,
    conv_input,
    conv_taps,
    out_proj,
):
    n_sp = lax.axis_size(SP)
    n_z, n_c, n_y, n_x = (lax.axis_size(a) for a in ("z", "c", "y", "x"))
    n_tp = n_y * n_x
    tokens, top = route_ids.shape
    width = moe_input.shape[1]
    wdev = width // n_tp
    wy = width // n_y
    chunks = wy // wdev
    hidden = gate_weight.shape[1]
    experts = n_sp
    cap = 5 * tokens // (2 * experts)
    kx = cap // n_x
    slots = experts * kx
    yi = lax.axis_index("y")
    xi = lax.axis_index("x")

    weights = jnp.concatenate([gate_weight, lin_weight, down_weight], axis=0)
    blocks = [weights] + [turned(weights, "x", d) for d in range(1, n_x)]

    flat = route_ids.reshape(-1)
    order = jnp.arange(flat.shape[0], dtype=jnp.int32)
    same = (flat[:, None] == flat[None, :]) & (order[None, :] < order[:, None])
    rank = jnp.sum(same.astype(jnp.int32), axis=1)
    position = (flat * cap + rank).reshape(tokens, top)
    first, second = position[:, 0], position[:, 1]

    mine = jnp.arange(slots, dtype=jnp.int32)
    mine = (mine // kx) * cap + xi * kx + mine % kx
    hit0 = mine[:, None] == first[None, :]
    hit1 = mine[:, None] == second[None, :]
    pick = (hit0 | hit1).astype(BF)
    slot_weight = jnp.sum(
        jnp.where(hit0, route_weights[:, 0][None, :], 0.0)
        + jnp.where(hit1, route_weights[:, 1][None, :], 0.0),
        axis=1,
    )
    my_rows = lax.dynamic_slice_in_dim(moe_input, yi * wy, wy, 1)
    my_grads = lax.dynamic_slice_in_dim(out_grad, yi * wy, wy, 1)
    send_rows = dot(pick, my_rows, 1, 0).astype(BF)
    send_grads = (slot_weight[:, None] * dot(pick, my_grads, 1, 0)).astype(BF)
    send = jnp.concatenate(
        [a.reshape(experts, kx, chunks, wdev) for a in (send_rows, send_grads)], axis=2
    )
    got = swap(send.reshape(experts, kx * 2 * chunks, wdev), SP)
    got = got.reshape(slots, 2 * chunks, wdev).transpose(1, 0, 2)
    got = from_everyone(got, "y").reshape(n_y, 2, chunks, slots, wdev)
    both = got.transpose(1, 3, 0, 2, 4).reshape(2, slots, width)
    rows, grads = both[0], both[1]

    gate_w, lin_w, down_w = (jnp.concatenate([b[k] for b in blocks], axis=0) for k in range(3))
    act, gate_cot, lin_cot = expert_cots(rows, grads, gate_w, lin_w, down_w)
    part = (dot(gate_cot, gate_w, 1, 0) + dot(lin_cot, lin_w, 1, 0)).astype(BF)
    part = part.reshape(slots, n_tp, wdev).transpose(1, 0, 2)
    part = swap(part, TP).reshape(n_y, n_x, experts, kx, wdev)
    slot_sums = jnp.sum(part.astype(F32), axis=0).astype(BF)
    slot_sums = slot_sums.transpose(1, 0, 2, 3).reshape(experts, cap, wdev)
    returned = swap(slot_sums, SP).reshape(experts * cap, wdev)

    terms = jnp.stack(
        [
            dot(cot, other, 0, 0).astype(BF).reshape(n_x, hidden, width)
            for cot, other in ((gate_cot, rows), (lin_cot, rows), (act, grads))
        ],
        axis=1,
    )
    total = terms[0].astype(F32)
    for d in range(1, n_x):
        total = total + turned(terms[d], "x", -d).astype(F32)
    weight_grads = total.astype(BF)
    gate_grad, lin_grad, down_grad = (weight_grads[k : k + 1] for k in range(3))

    every = jnp.arange(experts * cap, dtype=jnp.int32)[None, :]
    place = ((first[:, None] == every) | (second[:, None] == every)).astype(BF)
    row_grads = dot(place, returned, 1, 0).astype(BF)
    full_rows = from_everyone(row_grads, TP).transpose(1, 0, 2).reshape(tokens, width)
    stream_grad = (out_grad.astype(F32) + full_rows.astype(F32)).astype(BF)

    taps = conv_taps.shape[0]
    conv_values = (inner_gate.astype(F32) * conv_input.astype(F32)).astype(BF)
    prior_rows = from_behind(conv_values[tokens - (taps - 1) :], SP, 1)
    extended = jnp.concatenate([prior_rows, conv_values], axis=0).astype(F32)
    convolved = jnp.zeros((tokens, wdev), F32)
    for tap in range(taps):
        convolved = convolved + conv_taps[tap][None, :] * extended[tap : tap + tokens]
    mixed = (outer_gate.astype(F32) * convolved).astype(BF)

    proj = doubled(doubled(out_proj.T, "z"), "c").reshape(width, wdev)
    mixed_grad = dot(stream_grad, proj, 1, 0)
    terms = dot(stream_grad, mixed, 0, 0).astype(BF).reshape(n_z, n_c, -1, wdev)
    terms = swap(terms.transpose(1, 0, 2, 3), "c")
    terms = jnp.sum(terms.astype(F32), axis=0).astype(BF)
    out_proj_grad = jnp.sum(swap(terms, "z").astype(F32), axis=0)

    outer_gate_grad = (mixed_grad * convolved).astype(BF)
    conv_cot = (mixed_grad * outer_gate.astype(F32)).astype(BF)
    later_rows = from_behind(conv_cot[: taps - 1], SP, -1)
    extended_cot = jnp.concatenate([conv_cot, later_rows], axis=0).astype(F32)
    value_grad = jnp.zeros((tokens, wdev), F32)
    for tap in range(taps):
        start = taps - 1 - tap
        value_grad = value_grad + conv_taps[tap][None, :] * extended_cot[start : start + tokens]
    inner_gate_grad = (value_grad * conv_input.astype(F32)).astype(BF)
    conv_input_grad = (value_grad * inner_gate.astype(F32)).astype(BF)
    return (
        gate_grad,
        lin_grad,
        down_grad,
        out_proj_grad,
        outer_gate_grad,
        inner_gate_grad,
        conv_input_grad,
    )


def solution(mesh):
    torus = Mesh(mesh.devices.reshape(-1, 2, 4, 4), ("z", "c", "y", "x"))
    tokens = P(SP, None)
    expert = P(SP, TP, None)
    mixer = P(SP, TP)
    return jax.shard_map(
        local,
        mesh=torus,
        in_specs=(tokens,) * 4 + (expert,) * 3 + (mixer,) * 3 + (P(None, TP), P(TP, SP)),
        out_specs=(expert,) * 3 + (mixer,) * 4,
        check_vma=False,
    )
```

```python
import functools

import jax
import jax.numpy as jnp
from jax import lax
from jax.experimental import pallas as pl
from jax.experimental.pallas import tpu as pltpu
from jax.sharding import Mesh
from jax.sharding import PartitionSpec as P


SP = ("z", "c")
TP = ("y", "x")
LIMIT = 7.0
ALPHA = 1.702
LANES = 128
BF = jnp.bfloat16
F32 = jnp.float32


def swap(blocks, axis):
    return lax.all_to_all(blocks, axis, split_axis=0, concat_axis=0, tiled=True)


def turned(value, axis, by):
    count = lax.axis_size(axis)
    return lax.ppermute(value, axis, [(i, (i + by) % count) for i in range(count)])


def mirrored(value, axis, bit):
    return lax.ppermute(value, axis, [(i, i ^ bit) for i in range(lax.axis_size(axis))])


def doubled(value, axis):
    index = lax.axis_index(axis)
    bit = lax.axis_size(axis) // 2
    while bit:
        other = mirrored(value, axis, bit)
        high = (index & bit) > 0
        both = (jnp.where(high, other, value), jnp.where(high, value, other))
        value = jnp.stack(both, axis=value.ndim - 2)
        bit //= 2
    return value


def from_behind(value, axis, by):
    count = lax.axis_size(axis)
    pairs = [(i, i + by) for i in range(count) if 0 <= i + by < count]
    return lax.ppermute(value, axis, pairs)


def dot(a, b, ca, cb):
    return lax.dot_general(a, b, (((ca,), (cb,)), ((), ())), preferred_element_type=F32)


def expert_cots(rows, grads, gate_w, lin_w, down_w):
    gate_pre = dot(rows, gate_w, 1, 1)
    lin_pre = dot(rows, lin_w, 1, 1)
    act_grad = dot(grads, down_w, 1, 1)
    gate_cut = jnp.minimum(gate_pre, LIMIT)
    lin_cut = jnp.clip(lin_pre, -LIMIT, LIMIT)
    sigma = jax.nn.sigmoid(ALPHA * gate_cut)
    act = (gate_cut * sigma * (lin_cut + 1.0)).astype(BF)
    slope = sigma * (1.0 + ALPHA * gate_cut * (1.0 - sigma))
    gate_cot = jnp.where(gate_pre < LIMIT, act_grad * (lin_cut + 1.0) * slope, 0.0).astype(BF)
    lin_cot = jnp.where(jnp.abs(lin_pre) < LIMIT, act_grad * gate_cut * sigma, 0.0).astype(BF)
    return act, gate_cot, lin_cot


def routing_kernel(yi_ref, xi_ref, ids_ref, weights_ref, rows_ref, grads_ref, send_ref, place_ref, *, kx, cap, padded):
    tokens = ids_ref.shape[1]
    experts = send_ref.shape[0] // kx
    ids = ids_ref[...]
    expert = lax.broadcasted_iota(jnp.int32, (experts, tokens), 0)
    first = expert == ids[0:1, :]
    second = expert == ids[1:2, :]
    one = jnp.where(first | second, 1.0, 0.0).astype(BF)
    early = lax.broadcasted_iota(jnp.int32, (tokens, tokens), 0)
    late = lax.broadcasted_iota(jnp.int32, (tokens, tokens), 1)
    before = dot(one, jnp.where(early < late, 1.0, 0.0).astype(BF), 1, 0)
    rank0 = jnp.sum(jnp.where(first, before, 0.0), axis=0, keepdims=True).astype(jnp.int32)
    rank1 = jnp.sum(jnp.where(second, before, 0.0), axis=0, keepdims=True).astype(jnp.int32)
    place_ref[0:1, :] = ids[0:1, :] * padded + rank0
    place_ref[1:2, :] = ids[1:2, :] * padded + rank1
    slots = experts * kx
    slot = lax.broadcasted_iota(jnp.int32, (slots, tokens), 0)
    owner = slot // kx
    slot = owner * cap + xi_ref[0] * kx + (slot - owner * kx)
    hit0 = slot == ids[0:1, :] * cap + rank0
    hit1 = slot == ids[1:2, :] * cap + rank1
    pick = jnp.where(hit0 | hit1, 1.0, 0.0).astype(BF)
    w = weights_ref[...]
    weight = jnp.sum(
        jnp.where(hit0, w[0:1, :], 0.0) + jnp.where(hit1, w[1:2, :], 0.0), axis=1, keepdims=True
    )
    rows = dot(pick, rows_ref[...], 1, 0)
    grads = weight * dot(pick, grads_ref[...], 1, 0)
    both = jnp.concatenate([rows, grads], axis=1)
    send_ref[...] = both.reshape(slots, both.shape[1] // LANES, LANES).astype(BF)


def route(route_ids, route_weights, moe_input, out_grad, yi, xi, n_y, kx, experts, cap, padded):
    tokens, width = moe_input.shape
    wy = width // n_y
    slots = experts * kx
    return pl.pallas_call(
        functools.partial(routing_kernel, kx=kx, cap=cap, padded=padded),
        grid_spec=pltpu.PrefetchScalarGridSpec(
            num_scalar_prefetch=2,
            grid=(1,),
            in_specs=[
                pl.BlockSpec((2, tokens), lambda i, y, x: (0, 0)),
                pl.BlockSpec((2, tokens), lambda i, y, x: (0, 0)),
                pl.BlockSpec((tokens, wy), lambda i, y, x: (0, y[0])),
                pl.BlockSpec((tokens, wy), lambda i, y, x: (0, y[0])),
            ],
            out_specs=[
                pl.BlockSpec((slots, 2 * wy // LANES, LANES), lambda i, y, x: (0, 0, 0)),
                pl.BlockSpec((2, tokens), lambda i, y, x: (0, 0)),
            ],
        ),
        out_shape=[
            jax.ShapeDtypeStruct((slots, 2 * wy // LANES, LANES), BF),
            jax.ShapeDtypeStruct((2, tokens), jnp.int32),
        ],
        name="route",
    )(yi[None], xi[None], route_ids.T, route_weights.T, moe_input, out_grad)


def regroup_kernel(got_ref, out_ref):
    _, both, _ = got_ref.shape
    got = got_ref[...].astype(F32)
    for f in range(both):
        piece = got[:, f, :].astype(BF)
        for y in range(out_ref.shape[0]):
            out_ref[y, f] = piece


def expert_kernel(got_ref, w0_ref, w1_ref, w2_ref, w3_ref, part_ref, cots_ref):
    n_y, both, _, lanes = got_ref.shape
    chunks = both // 2
    rows = jnp.concatenate([got_ref[y, f] for y in range(n_y) for f in range(chunks)], axis=1)
    grads = jnp.concatenate(
        [got_ref[y, chunks + f] for y in range(n_y) for f in range(chunks)], axis=1
    )
    refs = (w0_ref, w1_ref, w2_ref, w3_ref)
    gate_w, lin_w, down_w = (jnp.concatenate([r[k] for r in refs], axis=0) for k in range(3))
    act, gate_cot, lin_cot = expert_cots(rows, grads, gate_w, lin_w, down_w)
    cots_ref[0] = gate_cot
    cots_ref[1] = lin_cot
    cots_ref[2] = act
    part = dot(gate_cot, gate_w, 1, 0) + dot(lin_cot, lin_w, 1, 0)
    for t in range(part_ref.shape[0]):
        part_ref[t] = part[:, t * lanes : (t + 1) * lanes].astype(BF)


def weight_grad_kernel(got_ref, cots_ref, o0_ref, o1_ref, o2_ref, o3_ref):
    n_y, both, _, _ = got_ref.shape
    chunks = both // 2
    outs = (o0_ref, o1_ref, o2_ref, o3_ref)
    hidden = o0_ref.shape[1]
    for k in range(3):
        offset = chunks if k == 2 else 0
        other = jnp.concatenate(
            [got_ref[y, offset + f] for y in range(n_y) for f in range(chunks)], axis=1
        )
        terms = dot(cots_ref[k], other, 0, 0)
        for d, ref in enumerate(outs):
            ref[k] = terms[d * hidden : (d + 1) * hidden].astype(ref.dtype)


def slot_sum_kernel(part_ref, out_ref, *, n_y, n_x, kx, padded):
    _, slots, lanes = part_ref.shape
    rows = out_ref.shape[0]
    cols = n_x * slots
    row = lax.broadcasted_iota(jnp.int32, (rows, cols), 0)
    col = lax.broadcasted_iota(jnp.int32, (rows, cols), 1)
    owner = row // padded
    at = row - owner * padded
    group = at // kx
    wanted = jnp.where(group < n_x, group * slots + owner * kx + (at - group * kx), -1)
    pick = jnp.where(wanted == col, 1.0, 0.0).astype(BF)
    total = jnp.zeros((rows, lanes), F32)
    for y in range(n_y):
        group_rows = jnp.concatenate([part_ref[y * n_x + x] for x in range(n_x)], axis=0)
        total = total + dot(pick, group_rows, 1, 0)
    out_ref[...] = total.astype(BF)


def combine_kernel(place_ref, back_ref, out_ref):
    tokens = place_ref.shape[1]
    every = lax.broadcasted_iota(jnp.int32, (back_ref.shape[0], tokens), 0)
    place = place_ref[...]
    hit = (every == place[0:1, :]) | (every == place[1:2, :])
    row_grads = dot(jnp.where(hit, 1.0, 0.0).astype(BF), back_ref[...], 0, 0).astype(BF)
    for t in range(out_ref.shape[0]):
        out_ref[t] = row_grads


def mixer_kernel(full_ref, out_grad_ref, proj_ref, mixed_ref, convolved_ref, outer_ref, terms_ref, outer_grad_ref, cot_ref):
    n_tp, _, _ = full_ref.shape
    n_c, n_z, per, _ = terms_ref.shape
    full = jnp.concatenate([full_ref[t] for t in range(n_tp)], axis=1)
    stream = (out_grad_ref[...].astype(F32) + full.astype(F32)).astype(BF)
    terms = dot(stream, mixed_ref[...], 0, 0).astype(BF)
    for z in range(n_z):
        for c in range(n_c):
            at = (z * n_c + c) * per
            terms_ref[c, z] = terms[at : at + per]
    mixed_grad = dot(stream, proj_ref[...], 1, 0)
    outer_grad_ref[...] = (mixed_grad * convolved_ref[...]).astype(BF)
    cot_ref[...] = (mixed_grad * outer_ref[...].astype(F32)).astype(BF)


def on_core(kernel, outs, *args, **static):
    return pl.pallas_call(
        functools.partial(kernel, **static) if static else kernel,
        out_shape=[jax.ShapeDtypeStruct(s, t) for s, t in outs],
    )(*args)


def local(
    moe_input,
    out_grad,
    route_ids,
    route_weights,
    gate_weight,
    lin_weight,
    down_weight,
    outer_gate,
    inner_gate,
    conv_input,
    conv_taps,
    out_proj,
):
    n_sp = lax.axis_size(SP)
    n_z, n_c, n_y, n_x = (lax.axis_size(a) for a in ("z", "c", "y", "x"))
    n_tp = n_y * n_x
    tokens, _ = route_ids.shape
    width = moe_input.shape[1]
    wdev = width // n_tp
    wy = width // n_y
    chunks = wy // wdev
    hidden = gate_weight.shape[1]
    experts = n_sp
    cap = 5 * tokens // (2 * experts)
    kx = cap // n_x
    slots = experts * kx
    padded = -(-cap // 8) * 8
    yi = lax.axis_index("y")
    xi = lax.axis_index("x")

    weights = jnp.concatenate([gate_weight, lin_weight, down_weight], axis=0)
    blocks = [weights] + [turned(weights, "x", d) for d in range(1, n_x)]

    send, place = route(
        route_ids, route_weights, moe_input, out_grad, yi, xi, n_y, kx, experts, cap, padded
    )
    got = swap(send.reshape(experts, kx * 2 * chunks, wdev), SP)
    (got,) = on_core(
        regroup_kernel, [((n_y, 2 * chunks, slots, wdev), BF)], got.reshape(slots, 2 * chunks, wdev)
    )
    got = swap(got, "y")

    part, cots = on_core(
        expert_kernel, [((n_tp, slots, wdev), BF), ((3, slots, n_x * hidden), BF)], got, *blocks
    )
    part = swap(part, TP)
    terms = on_core(weight_grad_kernel, [((3, hidden, width), BF)] * n_x, got, cots)
    (slot_sums,) = on_core(
        slot_sum_kernel,
        [((experts * padded, wdev), BF)],
        part,
        n_y=n_y,
        n_x=n_x,
        kx=kx,
        padded=padded,
    )
    back = swap(slot_sums.reshape(experts, padded, wdev), SP)
    back = back.reshape(experts * padded, wdev)

    total = terms[0].astype(F32)
    for d in range(1, n_x):
        total = total + turned(terms[d], "x", -d).astype(F32)
    weight_grads = total.astype(BF)
    gate_grad, lin_grad, down_grad = (weight_grads[k : k + 1] for k in range(3))

    (row_grads,) = on_core(combine_kernel, [((n_tp, tokens, wdev), BF)], place, back)
    full = swap(row_grads, TP)

    taps = conv_taps.shape[0]
    conv_values = (inner_gate.astype(F32) * conv_input.astype(F32)).astype(BF)
    prior_rows = from_behind(conv_values[tokens - (taps - 1) :], SP, 1)
    extended = jnp.concatenate([prior_rows, conv_values], axis=0).astype(F32)
    convolved = jnp.zeros((tokens, wdev), F32)
    for tap in range(taps):
        convolved = convolved + conv_taps[tap][None, :] * extended[tap : tap + tokens]
    mixed = (outer_gate.astype(F32) * convolved).astype(BF)

    proj = doubled(doubled(out_proj.T, "z"), "c").reshape(width, wdev)
    pair, outer_gate_grad, conv_cot = on_core(
        mixer_kernel,
        [((n_c, n_z, width // n_sp, wdev), BF), ((tokens, wdev), BF), ((tokens, wdev), BF)],
        full,
        out_grad,
        proj,
        mixed,
        convolved,
        outer_gate,
    )
    terms = swap(pair, "c")
    terms = jnp.sum(terms.astype(F32), axis=0).astype(BF)
    out_proj_grad = jnp.sum(swap(terms, "z").astype(F32), axis=0)

    later_rows = from_behind(conv_cot[: taps - 1], SP, -1)
    extended_cot = jnp.concatenate([conv_cot, later_rows], axis=0).astype(F32)
    value_grad = jnp.zeros((tokens, wdev), F32)
    for tap in range(taps):
        start = taps - 1 - tap
        value_grad = value_grad + conv_taps[tap][None, :] * extended_cot[start : start + tokens]
    inner_gate_grad = (value_grad * conv_input.astype(F32)).astype(BF)
    conv_input_grad = (value_grad * inner_gate.astype(F32)).astype(BF)
    return (
        gate_grad,
        lin_grad,
        down_grad,
        out_proj_grad,
        outer_gate_grad,
        inner_gate_grad,
        conv_input_grad,
    )


def solution(mesh):
    torus = Mesh(mesh.devices.reshape(-1, 2, 4, 4), ("z", "c", "y", "x"))
    tokens = P(SP, None)
    expert = P(SP, TP, None)
    mixer = P(SP, TP)
    return jax.shard_map(
        local,
        mesh=torus,
        in_specs=(tokens,) * 4 + (expert,) * 3 + (mixer,) * 3 + (P(None, TP), P(TP, SP)),
        out_specs=(expert,) * 3 + (mixer,) * 4,
        check_vma=False,
    )
```

```python
import functools

import jax
import jax.numpy as jnp
from jax import lax
from jax.experimental import pallas as pl
from jax.experimental.pallas import tpu as pltpu
from jax.sharding import Mesh
from jax.sharding import PartitionSpec as P


SP = ("z", "c")
TP = ("y", "x")
LIMIT = 7.0
ALPHA = 1.702
LANES = 128
BF = jnp.bfloat16
F32 = jnp.float32


def swap(blocks, axis):
    return lax.all_to_all(blocks, axis, split_axis=0, concat_axis=0, tiled=True)


def turned(value, axis, by):
    count = lax.axis_size(axis)
    return lax.ppermute(value, axis, [(i, (i + by) % count) for i in range(count)])


def mirrored(value, axis, bit):
    return lax.ppermute(value, axis, [(i, i ^ bit) for i in range(lax.axis_size(axis))])


def doubled(value, axis):
    index = lax.axis_index(axis)
    bit = lax.axis_size(axis) // 2
    while bit:
        other = mirrored(value, axis, bit)
        high = (index & bit) > 0
        both = (jnp.where(high, other, value), jnp.where(high, value, other))
        value = jnp.stack(both, axis=value.ndim - 2)
        bit //= 2
    return value


def from_behind(value, axis, by):
    count = lax.axis_size(axis)
    pairs = [(i, i + by) for i in range(count) if 0 <= i + by < count]
    return lax.ppermute(value, axis, pairs)


def dot(a, b, ca, cb):
    return lax.dot_general(a, b, (((ca,), (cb,)), ((), ())), preferred_element_type=F32)


def expert_cots(rows, grads, gate_w, lin_w, down_w):
    gate_pre = dot(rows, gate_w, 1, 1)
    lin_pre = dot(rows, lin_w, 1, 1)
    act_grad = dot(grads, down_w, 1, 1)
    gate_cut = jnp.minimum(gate_pre, LIMIT)
    lin_cut = jnp.clip(lin_pre, -LIMIT, LIMIT)
    sigma = jax.nn.sigmoid(ALPHA * gate_cut)
    act = (gate_cut * sigma * (lin_cut + 1.0)).astype(BF)
    slope = sigma * (1.0 + ALPHA * gate_cut * (1.0 - sigma))
    gate_cot = jnp.where(gate_pre < LIMIT, act_grad * (lin_cut + 1.0) * slope, 0.0).astype(BF)
    lin_cot = jnp.where(jnp.abs(lin_pre) < LIMIT, act_grad * gate_cut * sigma, 0.0).astype(BF)
    return act, gate_cot, lin_cot


def routing_kernel(yi_ref, xi_ref, ids_ref, weights_ref, rows_ref, grads_ref, send_ref, place_ref, *, kx, cap, padded):
    tokens = ids_ref.shape[1]
    experts = send_ref.shape[0] // kx
    ids = ids_ref[...]
    expert = lax.broadcasted_iota(jnp.int32, (experts, tokens), 0)
    first = expert == ids[0:1, :]
    second = expert == ids[1:2, :]
    one = jnp.where(first | second, 1.0, 0.0).astype(BF)
    early = lax.broadcasted_iota(jnp.int32, (tokens, tokens), 0)
    late = lax.broadcasted_iota(jnp.int32, (tokens, tokens), 1)
    before = dot(one, jnp.where(early < late, 1.0, 0.0).astype(BF), 1, 0)
    rank0 = jnp.sum(jnp.where(first, before, 0.0), axis=0, keepdims=True).astype(jnp.int32)
    rank1 = jnp.sum(jnp.where(second, before, 0.0), axis=0, keepdims=True).astype(jnp.int32)
    place_ref[0:1, :] = ids[0:1, :] * padded + rank0
    place_ref[1:2, :] = ids[1:2, :] * padded + rank1
    slots = experts * kx
    slot = lax.broadcasted_iota(jnp.int32, (slots, 1), 0)
    owner = slot // kx
    slot = owner * cap + xi_ref[0] * kx + (slot - owner * kx)
    hit0 = slot == ids[0:1, :] * cap + rank0
    hit1 = slot == ids[1:2, :] * cap + rank1
    pick = jnp.where(hit0 | hit1, 1.0, 0.0).astype(BF)
    w = weights_ref[...]
    weight = jnp.sum(
        jnp.where(hit0, w[0:1, :], 0.0) + jnp.where(hit1, w[1:2, :], 0.0), axis=1, keepdims=True
    )
    rows = dot(pick, rows_ref[...], 1, 0)
    grads = weight * dot(pick, grads_ref[...], 1, 0)
    both = jnp.concatenate([rows, grads], axis=1)
    send_ref[...] = both.reshape(slots, both.shape[1] // LANES, LANES).astype(BF)


def route(route_ids, route_weights, moe_input, out_grad, yi, xi, n_y, kx, experts, cap, padded):
    tokens, width = moe_input.shape
    wy = width // n_y
    slots = experts * kx
    return pl.pallas_call(
        functools.partial(routing_kernel, kx=kx, cap=cap, padded=padded),
        grid_spec=pltpu.PrefetchScalarGridSpec(
            num_scalar_prefetch=2,
            grid=(1,),
            in_specs=[
                pl.BlockSpec((2, tokens), lambda i, y, x: (0, 0)),
                pl.BlockSpec((2, tokens), lambda i, y, x: (0, 0)),
                pl.BlockSpec((tokens, wy), lambda i, y, x: (0, y[0])),
                pl.BlockSpec((tokens, wy), lambda i, y, x: (0, y[0])),
            ],
            out_specs=[
                pl.BlockSpec((slots, 2 * wy // LANES, LANES), lambda i, y, x: (0, 0, 0)),
                pl.BlockSpec((2, tokens), lambda i, y, x: (0, 0)),
            ],
        ),
        out_shape=[
            jax.ShapeDtypeStruct((slots, 2 * wy // LANES, LANES), BF),
            jax.ShapeDtypeStruct((2, tokens), jnp.int32),
        ],
        name="route",
    )(yi[None], xi[None], route_ids.T, route_weights.T, moe_input, out_grad)


def regroup_kernel(got_ref, out_ref):
    _, both, _ = got_ref.shape
    got = got_ref[...].astype(F32)
    for f in range(both):
        piece = got[:, f, :].astype(BF)
        for y in range(out_ref.shape[0]):
            out_ref[y, f] = piece


def expert_kernel(got_ref, w0_ref, w1_ref, w2_ref, w3_ref, part_ref, cots_ref):
    n_y, both, _, lanes = got_ref.shape
    chunks = both // 2
    rows = jnp.concatenate([got_ref[y, f] for y in range(n_y) for f in range(chunks)], axis=1)
    grads = jnp.concatenate(
        [got_ref[y, chunks + f] for y in range(n_y) for f in range(chunks)], axis=1
    )
    refs = (w0_ref, w1_ref, w2_ref, w3_ref)
    gate_w, lin_w, down_w = (jnp.concatenate([r[k] for r in refs], axis=0) for k in range(3))
    act, gate_cot, lin_cot = expert_cots(rows, grads, gate_w, lin_w, down_w)
    cots_ref[0] = gate_cot
    cots_ref[1] = lin_cot
    cots_ref[2] = act
    part = dot(gate_cot, gate_w, 1, 0) + dot(lin_cot, lin_w, 1, 0)
    for t in range(part_ref.shape[0]):
        part_ref[t] = part[:, t * lanes : (t + 1) * lanes].astype(BF)


def weight_grad_kernel(got_ref, cots_ref, o0_ref, o1_ref, o2_ref, o3_ref):
    n_y, both, _, _ = got_ref.shape
    chunks = both // 2
    outs = (o0_ref, o1_ref, o2_ref, o3_ref)
    hidden = o0_ref.shape[1]
    for k in range(3):
        offset = chunks if k == 2 else 0
        other = jnp.concatenate(
            [got_ref[y, offset + f] for y in range(n_y) for f in range(chunks)], axis=1
        )
        terms = dot(cots_ref[k], other, 0, 0)
        for d, ref in enumerate(outs):
            ref[k] = terms[d * hidden : (d + 1) * hidden].astype(ref.dtype)


def slot_sum_kernel(part_ref, out_ref, *, n_y, n_x, kx, padded):
    _, slots, _ = part_ref.shape
    rows = out_ref.shape[0]
    cols = n_x * slots
    row = lax.broadcasted_iota(jnp.int32, (rows, 1), 0)
    owner = row // padded
    at = row - owner * padded
    group = at // kx
    wanted = jnp.where(group < n_x, group * slots + owner * kx + (at - group * kx), -1)
    col = lax.broadcasted_iota(jnp.int32, (rows, cols), 1)
    pick = jnp.where(wanted == col, 1.0, 0.0).astype(BF)
    sums = []
    for x in range(n_x):
        total = part_ref[x].astype(F32)
        for y in range(1, n_y):
            total = total + part_ref[y * n_x + x].astype(F32)
        sums.append(total.astype(BF))
    out_ref[...] = dot(pick, jnp.concatenate(sums, axis=0), 1, 0).astype(BF)


def combine_kernel(place_ref, back_ref, out_ref):
    tokens = place_ref.shape[0]
    every = lax.broadcasted_iota(jnp.int32, (tokens, back_ref.shape[0]), 1)
    place = place_ref[...]
    hit = (every == place[:, 0:1]) | (every == place[:, 1:2])
    row_grads = dot(jnp.where(hit, 1.0, 0.0).astype(BF), back_ref[...], 1, 0).astype(BF)
    for t in range(out_ref.shape[0]):
        out_ref[t] = row_grads


def mixer_kernel(full_ref, out_grad_ref, proj_ref, mixed_ref, convolved_ref, outer_ref, terms_ref, outer_grad_ref, cot_ref):
    n_tp, _, _ = full_ref.shape
    n_c, n_z, per, _ = terms_ref.shape
    full = jnp.concatenate([full_ref[t] for t in range(n_tp)], axis=1)
    stream = (out_grad_ref[...].astype(F32) + full.astype(F32)).astype(BF)
    terms = dot(stream, mixed_ref[...], 0, 0).astype(BF)
    for z in range(n_z):
        for c in range(n_c):
            at = (z * n_c + c) * per
            terms_ref[c, z] = terms[at : at + per]
    mixed_grad = dot(stream, proj_ref[...], 1, 0)
    outer_grad_ref[...] = (mixed_grad * convolved_ref[...]).astype(BF)
    cot_ref[...] = (mixed_grad * outer_ref[...].astype(F32)).astype(BF)


def on_core(kernel, outs, *args, mib=12, **static):
    return pl.pallas_call(
        functools.partial(kernel, **static) if static else kernel,
        out_shape=[jax.ShapeDtypeStruct(s, t) for s, t in outs],
        compiler_params=pltpu.CompilerParams(vmem_limit_bytes=mib << 20),
    )(*args)


def local(
    moe_input,
    out_grad,
    route_ids,
    route_weights,
    gate_weight,
    lin_weight,
    down_weight,
    outer_gate,
    inner_gate,
    conv_input,
    conv_taps,
    out_proj,
):
    n_sp = lax.axis_size(SP)
    n_z, n_c, n_y, n_x = (lax.axis_size(a) for a in ("z", "c", "y", "x"))
    n_tp = n_y * n_x
    tokens, _ = route_ids.shape
    width = moe_input.shape[1]
    wdev = width // n_tp
    wy = width // n_y
    chunks = wy // wdev
    hidden = gate_weight.shape[1]
    experts = n_sp
    cap = 5 * tokens // (2 * experts)
    kx = cap // n_x
    slots = experts * kx
    padded = -(-cap // 8) * 8
    yi = lax.axis_index("y")
    xi = lax.axis_index("x")

    weights = jnp.concatenate([gate_weight, lin_weight, down_weight], axis=0)
    blocks = [weights] + [turned(weights, "x", d) for d in range(1, n_x)]

    send, place = route(
        route_ids, route_weights, moe_input, out_grad, yi, xi, n_y, kx, experts, cap, padded
    )
    got = swap(send.reshape(experts, kx * 2 * chunks, wdev), SP)
    (got,) = on_core(
        regroup_kernel, [((n_y, 2 * chunks, slots, wdev), BF)], got.reshape(slots, 2 * chunks, wdev)
    )
    got = swap(got, "y")

    part, cots = on_core(
        expert_kernel,
        [((n_tp, slots, wdev), BF), ((3, slots, n_x * hidden), BF)],
        got,
        *blocks,
        mib=24,
    )
    part = swap(part, TP)
    terms = on_core(weight_grad_kernel, [((3, hidden, width), BF)] * n_x, got, cots, mib=24)
    (slot_sums,) = on_core(
        slot_sum_kernel,
        [((experts * padded, wdev), BF)],
        part,
        n_y=n_y,
        n_x=n_x,
        kx=kx,
        padded=padded,
    )
    back = swap(slot_sums.reshape(experts, padded, wdev), SP)
    back = back.reshape(experts * padded, wdev)

    spread = [terms[0]] + [turned(terms[d], "x", -d) for d in range(1, n_x)]
    gate_grad, lin_grad, down_grad = (
        sum(t[k : k + 1].astype(F32) for t in spread).astype(BF) for k in range(3)
    )

    (row_grads,) = on_core(combine_kernel, [((n_tp, tokens, wdev), BF)], place.T, back)
    full = swap(row_grads, TP)

    taps = conv_taps.shape[0]
    conv_values = (inner_gate.astype(F32) * conv_input.astype(F32)).astype(BF)
    prior_rows = from_behind(conv_values[tokens - (taps - 1) :], SP, 1)
    extended = jnp.concatenate([prior_rows, conv_values], axis=0).astype(F32)
    convolved = jnp.zeros((tokens, wdev), F32)
    for tap in range(taps):
        convolved = convolved + conv_taps[tap][None, :] * extended[tap : tap + tokens]
    mixed = (outer_gate.astype(F32) * convolved).astype(BF)

    proj = doubled(doubled(out_proj.T, "z"), "c").reshape(width, wdev)
    pair, outer_gate_grad, conv_cot = on_core(
        mixer_kernel,
        [((n_c, n_z, width // n_sp, wdev), BF), ((tokens, wdev), BF), ((tokens, wdev), BF)],
        full,
        out_grad,
        proj,
        mixed,
        convolved,
        outer_gate,
    )
    terms = swap(pair, "c")
    terms = jnp.sum(terms.astype(F32), axis=0).astype(BF)
    out_proj_grad = jnp.sum(swap(terms, "z").astype(F32), axis=0)

    later_rows = from_behind(conv_cot[: taps - 1], SP, -1)
    extended_cot = jnp.concatenate([conv_cot, later_rows], axis=0).astype(F32)
    value_grad = jnp.zeros((tokens, wdev), F32)
    for tap in range(taps):
        start = taps - 1 - tap
        value_grad = value_grad + conv_taps[tap][None, :] * extended_cot[start : start + tokens]
    inner_gate_grad = (value_grad * conv_input.astype(F32)).astype(BF)
    conv_input_grad = (value_grad * inner_gate.astype(F32)).astype(BF)
    return (
        gate_grad,
        lin_grad,
        down_grad,
        out_proj_grad,
        outer_gate_grad,
        inner_gate_grad,
        conv_input_grad,
    )


def solution(mesh):
    torus = Mesh(mesh.devices.reshape(-1, 2, 4, 4), ("z", "c", "y", "x"))
    tokens = P(SP, None)
    expert = P(SP, TP, None)
    mixer = P(SP, TP)
    return jax.shard_map(
        local,
        mesh=torus,
        in_specs=(tokens,) * 4 + (expert,) * 3 + (mixer,) * 3 + (P(None, TP), P(TP, SP)),
        out_specs=(expert,) * 3 + (mixer,) * 4,
        check_vma=False,
    )
```

```python
import functools

import jax
import jax.numpy as jnp
from jax import lax
from jax.experimental import pallas as pl
from jax.experimental.pallas import tpu as pltpu
from jax.sharding import Mesh
from jax.sharding import PartitionSpec as P


SP = ("z", "c")
TP = ("y", "x")
LIMIT = 7.0
ALPHA = 1.702
LANES = 128
BF = jnp.bfloat16
F32 = jnp.float32


def swap(blocks, axis):
    return lax.all_to_all(blocks, axis, split_axis=0, concat_axis=0, tiled=True)


def turned(value, axis, by):
    count = lax.axis_size(axis)
    return lax.ppermute(value, axis, [(i, (i + by) % count) for i in range(count)])


def mirrored(value, axis, bit):
    return lax.ppermute(value, axis, [(i, i ^ bit) for i in range(lax.axis_size(axis))])


def doubled(value, axis):
    index = lax.axis_index(axis)
    bit = lax.axis_size(axis) // 2
    while bit:
        other = mirrored(value, axis, bit)
        high = (index & bit) > 0
        both = (jnp.where(high, other, value), jnp.where(high, value, other))
        value = jnp.stack(both, axis=value.ndim - 2)
        bit //= 2
    return value


def from_behind(value, axis, by):
    count = lax.axis_size(axis)
    pairs = [(i, i + by) for i in range(count) if 0 <= i + by < count]
    return lax.ppermute(value, axis, pairs)


def dot(a, b, ca, cb):
    return lax.dot_general(a, b, (((ca,), (cb,)), ((), ())), preferred_element_type=F32)


def expert_cots(rows, grads, gate_w, lin_w, down_w):
    gate_pre = dot(rows, gate_w, 1, 1)
    lin_pre = dot(rows, lin_w, 1, 1)
    act_grad = dot(grads, down_w, 1, 1)
    gate_cut = jnp.minimum(gate_pre, LIMIT)
    lin_cut = jnp.clip(lin_pre, -LIMIT, LIMIT)
    sigma = jax.nn.sigmoid(ALPHA * gate_cut)
    act = (gate_cut * sigma * (lin_cut + 1.0)).astype(BF)
    slope = sigma * (1.0 + ALPHA * gate_cut * (1.0 - sigma))
    gate_cot = jnp.where(gate_pre < LIMIT, act_grad * (lin_cut + 1.0) * slope, 0.0).astype(BF)
    lin_cot = jnp.where(jnp.abs(lin_pre) < LIMIT, act_grad * gate_cut * sigma, 0.0).astype(BF)
    return act, gate_cot, lin_cot


def routing_kernel(yi_ref, xi_ref, ids_ref, weights_ref, rows_ref, grads_ref, send_ref, place_ref, *, kx, cap, padded):
    tokens = ids_ref.shape[1]
    experts = send_ref.shape[0] // kx
    ids = ids_ref[...]
    expert = lax.broadcasted_iota(jnp.int32, (experts, tokens), 0)
    first = expert == ids[0:1, :]
    second = expert == ids[1:2, :]
    one = jnp.where(first | second, 1.0, 0.0).astype(BF)
    early = lax.broadcasted_iota(jnp.int32, (tokens, tokens), 0)
    late = lax.broadcasted_iota(jnp.int32, (tokens, tokens), 1)
    before = dot(one, jnp.where(early < late, 1.0, 0.0).astype(BF), 1, 0)
    rank0 = jnp.sum(jnp.where(first, before, 0.0), axis=0, keepdims=True).astype(jnp.int32)
    rank1 = jnp.sum(jnp.where(second, before, 0.0), axis=0, keepdims=True).astype(jnp.int32)
    place_ref[0:1, :] = ids[0:1, :] * padded + rank0
    place_ref[1:2, :] = ids[1:2, :] * padded + rank1
    slots = experts * kx
    slot = lax.broadcasted_iota(jnp.int32, (slots, 1), 0)
    owner = slot // kx
    slot = owner * cap + xi_ref[0] * kx + (slot - owner * kx)
    hit0 = slot == ids[0:1, :] * cap + rank0
    hit1 = slot == ids[1:2, :] * cap + rank1
    pick = jnp.where(hit0 | hit1, 1.0, 0.0).astype(BF)
    w = weights_ref[...]
    weight = jnp.sum(
        jnp.where(hit0, w[0:1, :], 0.0) + jnp.where(hit1, w[1:2, :], 0.0), axis=1, keepdims=True
    )
    rows = dot(pick, rows_ref[...], 1, 0)
    grads = weight * dot(pick, grads_ref[...], 1, 0)
    both = jnp.concatenate([rows, grads], axis=1)
    send_ref[...] = both.reshape(slots, both.shape[1] // LANES, LANES).astype(BF)


def route(route_ids, route_weights, moe_input, out_grad, yi, xi, n_y, kx, experts, cap, padded):
    tokens, width = moe_input.shape
    wy = width // n_y
    slots = experts * kx
    return pl.pallas_call(
        functools.partial(routing_kernel, kx=kx, cap=cap, padded=padded),
        grid_spec=pltpu.PrefetchScalarGridSpec(
            num_scalar_prefetch=2,
            grid=(1,),
            in_specs=[
                pl.BlockSpec((2, tokens), lambda i, y, x: (0, 0)),
                pl.BlockSpec((2, tokens), lambda i, y, x: (0, 0)),
                pl.BlockSpec((tokens, wy), lambda i, y, x: (0, y[0])),
                pl.BlockSpec((tokens, wy), lambda i, y, x: (0, y[0])),
            ],
            out_specs=[
                pl.BlockSpec((slots, 2 * wy // LANES, LANES), lambda i, y, x: (0, 0, 0)),
                pl.BlockSpec((2, tokens), lambda i, y, x: (0, 0)),
            ],
        ),
        out_shape=[
            jax.ShapeDtypeStruct((slots, 2 * wy // LANES, LANES), BF),
            jax.ShapeDtypeStruct((2, tokens), jnp.int32),
        ],
        name="route",
    )(yi[None], xi[None], route_ids.T, route_weights.T, moe_input, out_grad)


def regroup_kernel(got_ref, out_ref):
    _, both, _ = got_ref.shape
    got = got_ref[...].astype(F32)
    for f in range(both):
        piece = got[:, f, :].astype(BF)
        for y in range(out_ref.shape[0]):
            out_ref[y, f] = piece


def expert_kernel(got_ref, w0_ref, w1_ref, w2_ref, w3_ref, part_ref, cots_ref):
    n_y, both, _, lanes = got_ref.shape
    chunks = both // 2
    rows = jnp.concatenate([got_ref[y, f] for y in range(n_y) for f in range(chunks)], axis=1)
    grads = jnp.concatenate(
        [got_ref[y, chunks + f] for y in range(n_y) for f in range(chunks)], axis=1
    )
    refs = (w0_ref, w1_ref, w2_ref, w3_ref)
    gate_w, lin_w, down_w = (jnp.concatenate([r[k] for r in refs], axis=0) for k in range(3))
    act, gate_cot, lin_cot = expert_cots(rows, grads, gate_w, lin_w, down_w)
    cots_ref[0] = gate_cot
    cots_ref[1] = lin_cot
    cots_ref[2] = act
    part = dot(gate_cot, gate_w, 1, 0) + dot(lin_cot, lin_w, 1, 0)
    for t in range(part_ref.shape[0]):
        part_ref[t] = part[:, t * lanes : (t + 1) * lanes].astype(BF)


def weight_grad_kernel(got_ref, cots_ref, o0_ref, o1_ref, o2_ref, o3_ref):
    n_y, both, _, _ = got_ref.shape
    chunks = both // 2
    outs = (o0_ref, o1_ref, o2_ref, o3_ref)
    hidden = o0_ref.shape[1]
    for k in range(3):
        offset = chunks if k == 2 else 0
        other = jnp.concatenate(
            [got_ref[y, offset + f] for y in range(n_y) for f in range(chunks)], axis=1
        )
        terms = dot(cots_ref[k], other, 0, 0)
        for d, ref in enumerate(outs):
            ref[k] = terms[d * hidden : (d + 1) * hidden].astype(ref.dtype)


def slot_sum_kernel(part_ref, out_ref, *, n_y, n_x, kx, padded):
    _, slots, _ = part_ref.shape
    rows = out_ref.shape[0]
    cols = n_x * slots
    row = lax.broadcasted_iota(jnp.int32, (rows, 1), 0)
    owner = row // padded
    at = row - owner * padded
    group = at // kx
    wanted = jnp.where(group < n_x, group * slots + owner * kx + (at - group * kx), -1)
    col = lax.broadcasted_iota(jnp.int32, (rows, cols), 1)
    pick = jnp.where(wanted == col, 1.0, 0.0).astype(BF)
    sums = []
    for x in range(n_x):
        total = part_ref[x].astype(F32)
        for y in range(1, n_y):
            total = total + part_ref[y * n_x + x].astype(F32)
        sums.append(total.astype(BF))
    out_ref[...] = dot(pick, jnp.concatenate(sums, axis=0), 1, 0).astype(BF)


def combine_kernel(place_ref, back_ref, out_ref):
    tokens = place_ref.shape[0]
    every = lax.broadcasted_iota(jnp.int32, (tokens, back_ref.shape[0]), 1)
    place = place_ref[...]
    hit = (every == place[:, 0:1]) | (every == place[:, 1:2])
    row_grads = dot(jnp.where(hit, 1.0, 0.0).astype(BF), back_ref[...], 1, 0).astype(BF)
    for t in range(out_ref.shape[0]):
        out_ref[t] = row_grads


def mixer_kernel(
    full_ref, out_grad_ref, proj_ref, mixed_hbm, convolved_hbm, outer_hbm,
    terms_ref, cot_ref, outer_grad_hbm,
    mixed_ref, convolved_ref, outer_ref, outer_grad_ref, sems,
):
    n_tp, _, _ = full_ref.shape
    n_c, n_z, per, _ = terms_ref.shape
    fetches = [
        pltpu.make_async_copy(src, dst, sems.at[i])
        for i, (src, dst) in enumerate(
            ((convolved_hbm, convolved_ref), (outer_hbm, outer_ref), (mixed_hbm, mixed_ref))
        )
    ]
    for fetch in fetches:
        fetch.start()
    full = jnp.concatenate([full_ref[t] for t in range(n_tp)], axis=1)
    stream = (out_grad_ref[...].astype(F32) + full.astype(F32)).astype(BF)
    mixed_grad = dot(stream, proj_ref[...], 1, 0)
    fetches[0].wait()
    outer_grad_ref[...] = (mixed_grad * convolved_ref[...]).astype(BF)
    keep = pltpu.make_async_copy(outer_grad_ref, outer_grad_hbm, sems.at[3])
    keep.start()
    fetches[1].wait()
    cot_ref[...] = (mixed_grad * outer_ref[...].astype(F32)).astype(BF)
    fetches[2].wait()
    terms = dot(stream, mixed_ref[...], 0, 0).astype(BF)
    for z in range(n_z):
        for c in range(n_c):
            at = (z * n_c + c) * per
            terms_ref[c, z] = terms[at : at + per]
    keep.wait()


def in_hbm(value):
    return pltpu.with_memory_space_constraint(value, pltpu.HBM)


def mix(full, out_grad, proj, mixed, convolved, outer_gate, n_c, n_z):
    _, tokens, lanes = full.shape
    small = (tokens, lanes)
    whole = pl.BlockSpec(memory_space=pltpu.VMEM)
    away = pl.BlockSpec(memory_space=pltpu.HBM)
    return pl.pallas_call(
        mixer_kernel,
        in_specs=[whole, whole, whole, away, away, away],
        out_specs=[whole, whole, away],
        out_shape=[
            pltpu.HBM((n_c, n_z, proj.shape[0] // (n_c * n_z), lanes), BF),
            pltpu.HBM(small, BF),
            pltpu.HBM(small, BF),
        ],
        scratch_shapes=[
            pltpu.VMEM(small, BF),
            pltpu.VMEM(small, F32),
            pltpu.VMEM(small, BF),
            pltpu.VMEM(small, BF),
            pltpu.SemaphoreType.DMA((4,)),
        ],
        compiler_params=pltpu.CompilerParams(vmem_limit_bytes=16 << 20),
        name="mixer",
    )(full, out_grad, proj, *map(in_hbm, (mixed, convolved, outer_gate)))


def on_core(kernel, outs, *args, mib=12, **static):
    return pl.pallas_call(
        functools.partial(kernel, **static) if static else kernel,
        out_shape=[pltpu.HBM(s, t) for s, t in outs],
        compiler_params=pltpu.CompilerParams(vmem_limit_bytes=mib << 20),
    )(*args)


def local(
    moe_input,
    out_grad,
    route_ids,
    route_weights,
    gate_weight,
    lin_weight,
    down_weight,
    outer_gate,
    inner_gate,
    conv_input,
    conv_taps,
    out_proj,
):
    n_sp = lax.axis_size(SP)
    n_z, n_c, n_y, n_x = (lax.axis_size(a) for a in ("z", "c", "y", "x"))
    n_tp = n_y * n_x
    tokens, _ = route_ids.shape
    width = moe_input.shape[1]
    wdev = width // n_tp
    wy = width // n_y
    chunks = wy // wdev
    hidden = gate_weight.shape[1]
    experts = n_sp
    cap = 5 * tokens // (2 * experts)
    kx = cap // n_x
    slots = experts * kx
    padded = -(-cap // 8) * 8
    yi = lax.axis_index("y")
    xi = lax.axis_index("x")

    weights = jnp.concatenate([gate_weight, lin_weight, down_weight], axis=0)
    blocks = [weights] + [turned(weights, "x", d) for d in range(1, n_x)]

    send, place = route(
        route_ids, route_weights, moe_input, out_grad, yi, xi, n_y, kx, experts, cap, padded
    )
    got = swap(send.reshape(experts, kx * 2 * chunks, wdev), SP)
    (got,) = on_core(
        regroup_kernel, [((n_y, 2 * chunks, slots, wdev), BF)], got.reshape(slots, 2 * chunks, wdev)
    )
    got = swap(got, "y")

    part, cots = on_core(
        expert_kernel,
        [((n_tp, slots, wdev), BF), ((3, slots, n_x * hidden), BF)],
        got,
        *blocks,
        mib=24,
    )
    part = swap(part, TP)
    terms = on_core(weight_grad_kernel, [((3, hidden, width), BF)] * n_x, got, cots, mib=24)
    (slot_sums,) = on_core(
        slot_sum_kernel,
        [((experts * padded, wdev), BF)],
        part,
        n_y=n_y,
        n_x=n_x,
        kx=kx,
        padded=padded,
    )
    back = swap(slot_sums.reshape(experts, padded, wdev), SP)
    back = back.reshape(experts * padded, wdev)

    spread = [terms[0]] + [turned(terms[d], "x", -d) for d in range(1, n_x)]
    gate_grad, lin_grad, down_grad = (
        sum(t[k : k + 1].astype(F32) for t in spread).astype(BF) for k in range(3)
    )

    (row_grads,) = on_core(combine_kernel, [((n_tp, tokens, wdev), BF)], place.T, back)
    full = swap(row_grads, TP)

    taps = conv_taps.shape[0]
    conv_values = (inner_gate.astype(F32) * conv_input.astype(F32)).astype(BF)
    prior_rows = from_behind(conv_values[tokens - (taps - 1) :], SP, 1)
    extended = jnp.concatenate([prior_rows, conv_values], axis=0).astype(F32)
    convolved = jnp.zeros((tokens, wdev), F32)
    for tap in range(taps):
        convolved = convolved + conv_taps[tap][None, :] * extended[tap : tap + tokens]
    mixed = (outer_gate.astype(F32) * convolved).astype(BF)

    proj = doubled(doubled(out_proj.T, "z"), "c").reshape(width, wdev)
    pair, conv_cot, outer_gate_grad = mix(
        full, out_grad, proj, mixed, convolved, outer_gate, n_c, n_z
    )
    terms = swap(pair, "c")
    terms = jnp.sum(terms.astype(F32), axis=0).astype(BF)
    out_proj_grad = jnp.sum(swap(terms, "z").astype(F32), axis=0)

    later_rows = from_behind(conv_cot[: taps - 1], SP, -1)
    extended_cot = jnp.concatenate([conv_cot, later_rows], axis=0).astype(F32)
    value_grad = jnp.zeros((tokens, wdev), F32)
    for tap in range(taps):
        start = taps - 1 - tap
        value_grad = value_grad + conv_taps[tap][None, :] * extended_cot[start : start + tokens]
    inner_gate_grad = (value_grad * conv_input.astype(F32)).astype(BF)
    conv_input_grad = (value_grad * inner_gate.astype(F32)).astype(BF)
    return (
        gate_grad,
        lin_grad,
        down_grad,
        out_proj_grad,
        outer_gate_grad,
        inner_gate_grad,
        conv_input_grad,
    )


def solution(mesh):
    torus = Mesh(mesh.devices.reshape(-1, 2, 4, 4), ("z", "c", "y", "x"))
    tokens = P(SP, None)
    expert = P(SP, TP, None)
    mixer = P(SP, TP)
    return jax.shard_map(
        local,
        mesh=torus,
        in_specs=(tokens,) * 4 + (expert,) * 3 + (mixer,) * 3 + (P(None, TP), P(TP, SP)),
        out_specs=(expert,) * 3 + (mixer,) * 4,
        check_vma=False,
    )
```

```python
import functools

import jax
import jax.numpy as jnp
from jax import lax
from jax.experimental import pallas as pl
from jax.experimental.pallas import tpu as pltpu
from jax.sharding import Mesh
from jax.sharding import PartitionSpec as P


SP = ("z", "c")
TP = ("y", "x")
LIMIT = 7.0
ALPHA = 1.702
LANES = 128
BF = jnp.bfloat16
F32 = jnp.float32


def swap(blocks, axis):
    return lax.all_to_all(blocks, axis, split_axis=0, concat_axis=0, tiled=True)


def turned(value, axis, by):
    count = lax.axis_size(axis)
    return lax.ppermute(value, axis, [(i, (i + by) % count) for i in range(count)])


def shifted(value, axis, group, stride, by):
    count = lax.axis_size(axis)
    size = group * stride

    def source(i):
        return i // size * size + (i + by * stride) % size

    return lax.ppermute(value, axis, [(source(i), i) for i in range(count)])


def grouped(value, axis, group, stride):
    others = [shifted(value, axis, group, stride, by) for by in range(1, group)]
    place = lax.rem(lax.div(lax.axis_index(axis), jnp.int32(stride)), jnp.int32(group))
    return ordered([value, *others], place)


def from_behind(value, axis, by):
    count = lax.axis_size(axis)
    pairs = [(i, i + by) for i in range(count) if 0 <= i + by < count]
    return lax.ppermute(value, axis, pairs)


def dot(a, b, ca, cb):
    return lax.dot_general(a, b, (((ca,), (cb,)), ((), ())), preferred_element_type=F32)


def expert_cots(rows, grads, gate_w, lin_w, down_w):
    gate_pre = dot(rows, gate_w, 1, 1)
    lin_pre = dot(rows, lin_w, 1, 1)
    act_grad = dot(grads, down_w, 1, 1)
    gate_cut = jnp.minimum(gate_pre, LIMIT)
    lin_cut = jnp.clip(lin_pre, -LIMIT, LIMIT)
    sigma = jax.nn.sigmoid(ALPHA * gate_cut)
    act = (gate_cut * sigma * (lin_cut + 1.0)).astype(BF)
    slope = sigma * (1.0 + ALPHA * gate_cut * (1.0 - sigma))
    gate_cot = jnp.where(gate_pre < LIMIT, act_grad * (lin_cut + 1.0) * slope, 0.0).astype(BF)
    lin_cot = jnp.where(jnp.abs(lin_pre) < LIMIT, act_grad * gate_cut * sigma, 0.0).astype(BF)
    return act, gate_cot, lin_cot


def routing_kernel(yi_ref, xi_ref, ids_ref, weights_ref, rows_ref, grads_ref, send_ref, place_ref, *, kx, cap, padded):
    tokens = ids_ref.shape[1]
    experts = send_ref.shape[0] // kx
    ids = ids_ref[...]
    expert = lax.broadcasted_iota(jnp.int32, (experts, tokens), 0)
    first = expert == ids[0:1, :]
    second = expert == ids[1:2, :]
    one = jnp.where(first | second, 1.0, 0.0).astype(BF)
    early = lax.broadcasted_iota(jnp.int32, (tokens, tokens), 0)
    late = lax.broadcasted_iota(jnp.int32, (tokens, tokens), 1)
    before = dot(one, jnp.where(early < late, 1.0, 0.0).astype(BF), 1, 0)
    rank0 = jnp.sum(jnp.where(first, before, 0.0), axis=0, keepdims=True).astype(jnp.int32)
    rank1 = jnp.sum(jnp.where(second, before, 0.0), axis=0, keepdims=True).astype(jnp.int32)
    place_ref[0:1, :] = ids[0:1, :] * padded + rank0
    place_ref[1:2, :] = ids[1:2, :] * padded + rank1
    slots = experts * kx
    slot = lax.broadcasted_iota(jnp.int32, (slots, 1), 0)
    owner = slot // kx
    slot = owner * cap + xi_ref[0] * kx + (slot - owner * kx)
    hit0 = slot == ids[0:1, :] * cap + rank0
    hit1 = slot == ids[1:2, :] * cap + rank1
    pick = jnp.where(hit0 | hit1, 1.0, 0.0).astype(BF)
    w = weights_ref[...]
    weight = jnp.sum(
        jnp.where(hit0, w[0:1, :], 0.0) + jnp.where(hit1, w[1:2, :], 0.0), axis=1, keepdims=True
    )
    rows = dot(pick, rows_ref[...], 1, 0)
    grads = weight * dot(pick, grads_ref[...], 1, 0)
    both = jnp.concatenate([rows, grads], axis=1)
    send_ref[...] = both.reshape(slots, both.shape[1] // LANES, LANES).astype(BF)


def route(route_ids, route_weights, moe_input, out_grad, yi, xi, n_y, kx, experts, cap, padded):
    tokens, width = moe_input.shape
    wy = width // n_y
    slots = experts * kx
    return pl.pallas_call(
        functools.partial(routing_kernel, kx=kx, cap=cap, padded=padded),
        grid_spec=pltpu.PrefetchScalarGridSpec(
            num_scalar_prefetch=2,
            grid=(1,),
            in_specs=[
                pl.BlockSpec((2, tokens), lambda i, y, x: (0, 0)),
                pl.BlockSpec((2, tokens), lambda i, y, x: (0, 0)),
                pl.BlockSpec((tokens, wy), lambda i, y, x: (0, y[0])),
                pl.BlockSpec((tokens, wy), lambda i, y, x: (0, y[0])),
            ],
            out_specs=[
                pl.BlockSpec((slots, 2 * wy // LANES, LANES), lambda i, y, x: (0, 0, 0)),
                pl.BlockSpec((2, tokens), lambda i, y, x: (0, 0)),
            ],
        ),
        out_shape=[
            jax.ShapeDtypeStruct((slots, 2 * wy // LANES, LANES), BF),
            jax.ShapeDtypeStruct((2, tokens), jnp.int32),
        ],
        name="route",
    )(yi[None], xi[None], route_ids.T, route_weights.T, moe_input, out_grad)


def regroup_kernel(got_ref, out_ref):
    _, both, _ = got_ref.shape
    got = got_ref[...].astype(F32)
    for f in range(both):
        piece = got[:, f, :].astype(BF)
        for y in range(out_ref.shape[0]):
            out_ref[y, f] = piece


def expert_kernel(got_ref, w0_ref, w1_ref, w2_ref, w3_ref, part_ref, cots_ref):
    n_y, both, _, lanes = got_ref.shape
    chunks = both // 2
    rows = jnp.concatenate([got_ref[y, f] for y in range(n_y) for f in range(chunks)], axis=1)
    grads = jnp.concatenate(
        [got_ref[y, chunks + f] for y in range(n_y) for f in range(chunks)], axis=1
    )
    refs = (w0_ref, w1_ref, w2_ref, w3_ref)
    gate_w, lin_w, down_w = (jnp.concatenate([r[k] for r in refs], axis=0) for k in range(3))
    act, gate_cot, lin_cot = expert_cots(rows, grads, gate_w, lin_w, down_w)
    cots_ref[0] = gate_cot
    cots_ref[1] = lin_cot
    cots_ref[2] = act
    part = dot(gate_cot, gate_w, 1, 0) + dot(lin_cot, lin_w, 1, 0)
    for t in range(part_ref.shape[0]):
        part_ref[t] = part[:, t * lanes : (t + 1) * lanes].astype(BF)


def weight_grad_kernel(got_ref, cots_ref, o0_ref, o1_ref, o2_ref, o3_ref):
    n_y, both, _, _ = got_ref.shape
    chunks = both // 2
    outs = (o0_ref, o1_ref, o2_ref, o3_ref)
    hidden = o0_ref.shape[1]
    for k in range(3):
        offset = chunks if k == 2 else 0
        other = jnp.concatenate(
            [got_ref[y, offset + f] for y in range(n_y) for f in range(chunks)], axis=1
        )
        terms = dot(cots_ref[k], other, 0, 0)
        for d, ref in enumerate(outs):
            ref[k] = terms[d * hidden : (d + 1) * hidden].astype(ref.dtype)


def slot_sum_kernel(part_ref, out_ref, *, n_y, n_x, kx, padded):
    _, slots, _ = part_ref.shape
    rows = out_ref.shape[0]
    cols = n_x * slots
    row = lax.broadcasted_iota(jnp.int32, (rows, 1), 0)
    owner = row // padded
    at = row - owner * padded
    group = at // kx
    wanted = jnp.where(group < n_x, group * slots + owner * kx + (at - group * kx), -1)
    col = lax.broadcasted_iota(jnp.int32, (rows, cols), 1)
    pick = jnp.where(wanted == col, 1.0, 0.0).astype(BF)
    sums = []
    for x in range(n_x):
        total = part_ref[x].astype(F32)
        for y in range(1, n_y):
            total = total + part_ref[y * n_x + x].astype(F32)
        sums.append(total.astype(BF))
    out_ref[...] = dot(pick, jnp.concatenate(sums, axis=0), 1, 0).astype(BF)


def combine_kernel(place_ref, back_ref, out_ref):
    tokens = place_ref.shape[0]
    every = lax.broadcasted_iota(jnp.int32, (tokens, back_ref.shape[0]), 1)
    place = place_ref[...]
    hit = (every == place[:, 0:1]) | (every == place[:, 1:2])
    row_grads = dot(jnp.where(hit, 1.0, 0.0).astype(BF), back_ref[...], 1, 0).astype(BF)
    for t in range(out_ref.shape[0]):
        out_ref[t] = row_grads


def mixer_kernel(
    full_ref, out_grad_ref, proj_ref, mixed_hbm, convolved_hbm, outer_hbm,
    terms_ref, cot_ref, outer_grad_hbm,
    mixed_ref, convolved_ref, outer_ref, outer_grad_ref, sems,
):
    n_tp, _, _ = full_ref.shape
    n_c, n_z, per, _ = terms_ref.shape
    fetches = [
        pltpu.make_async_copy(src, dst, sems.at[i])
        for i, (src, dst) in enumerate(
            ((convolved_hbm, convolved_ref), (outer_hbm, outer_ref), (mixed_hbm, mixed_ref))
        )
    ]
    for fetch in fetches:
        fetch.start()
    full = jnp.concatenate([full_ref[t] for t in range(n_tp)], axis=1)
    stream = (out_grad_ref[...].astype(F32) + full.astype(F32)).astype(BF)
    mixed_grad = dot(stream, proj_ref[...], 1, 0)
    fetches[0].wait()
    outer_grad_ref[...] = (mixed_grad * convolved_ref[...]).astype(BF)
    keep = pltpu.make_async_copy(outer_grad_ref, outer_grad_hbm, sems.at[3])
    keep.start()
    fetches[1].wait()
    cot_ref[...] = (mixed_grad * outer_ref[...].astype(F32)).astype(BF)
    fetches[2].wait()
    terms = dot(stream, mixed_ref[...], 0, 0).astype(BF)
    for z in range(n_z):
        for c in range(n_c):
            at = (z * n_c + c) * per
            terms_ref[c, z] = terms[at : at + per]
    keep.wait()


def order_kernel(place_ref, *refs):
    *parts, out_ref = refs
    for by, ref in enumerate(parts):
        at = place_ref[0] + by
        out_ref[jnp.where(at >= len(parts), at - len(parts), at)] = ref[...]


def ordered(parts, place):
    return pl.pallas_call(
        order_kernel,
        in_specs=[pl.BlockSpec(memory_space=pltpu.SMEM)]
        + [pl.BlockSpec(memory_space=pltpu.VMEM)] * len(parts),
        out_shape=jax.ShapeDtypeStruct((len(parts), *parts[0].shape), parts[0].dtype),
        compiler_params=pltpu.CompilerParams(vmem_limit_bytes=4 << 20),
    )(place[None], *parts)


def twin_kernel(place_ref, own_ref, other_ref, out_ref):
    near, far = own_ref.shape[:2]
    mine = place_ref[0]
    for f in range(far):
        for n in range(near):
            out_ref[f * near + n, mine] = own_ref[n, f]
            out_ref[f * near + n, 1 - mine] = other_ref[n, f]


def with_twin(own, other, place):
    near, far, *block = own.shape
    return pl.pallas_call(
        twin_kernel,
        in_specs=[pl.BlockSpec(memory_space=pltpu.SMEM)]
        + [pl.BlockSpec(memory_space=pltpu.VMEM)] * 2,
        out_shape=jax.ShapeDtypeStruct((far * near, 2, *block), own.dtype),
        compiler_params=pltpu.CompilerParams(vmem_limit_bytes=4 << 20),
        name="twins",
    )(place[None], own, other)


def in_hbm(value):
    return pltpu.with_memory_space_constraint(value, pltpu.HBM)


def mix(full, out_grad, proj, mixed, convolved, outer_gate, n_c, n_z):
    _, tokens, lanes = full.shape
    small = (tokens, lanes)
    whole = pl.BlockSpec(memory_space=pltpu.VMEM)
    away = pl.BlockSpec(memory_space=pltpu.HBM)
    return pl.pallas_call(
        mixer_kernel,
        in_specs=[whole, whole, whole, away, away, away],
        out_specs=[whole, whole, away],
        out_shape=[
            pltpu.HBM((n_c, n_z, proj.shape[0] // (n_c * n_z), lanes), BF),
            pltpu.HBM(small, BF),
            pltpu.HBM(small, BF),
        ],
        scratch_shapes=[
            pltpu.VMEM(small, BF),
            pltpu.VMEM(small, F32),
            pltpu.VMEM(small, BF),
            pltpu.VMEM(small, BF),
            pltpu.SemaphoreType.DMA((4,)),
        ],
        compiler_params=pltpu.CompilerParams(vmem_limit_bytes=16 << 20),
        name="mixer",
    )(full, out_grad, proj, *map(in_hbm, (mixed, convolved, outer_gate)))


def on_core(kernel, outs, *args, mib=12, **static):
    return pl.pallas_call(
        functools.partial(kernel, **static) if static else kernel,
        out_shape=[pltpu.HBM(s, t) for s, t in outs],
        compiler_params=pltpu.CompilerParams(vmem_limit_bytes=mib << 20),
    )(*args)


def local(
    moe_input,
    out_grad,
    route_ids,
    route_weights,
    gate_weight,
    lin_weight,
    down_weight,
    outer_gate,
    inner_gate,
    conv_input,
    conv_taps,
    out_proj,
):
    n_sp = lax.axis_size(SP)
    n_z, n_c, n_y, n_x = (lax.axis_size(a) for a in ("z", "c", "y", "x"))
    n_tp = n_y * n_x
    tokens, _ = route_ids.shape
    width = moe_input.shape[1]
    wdev = width // n_tp
    wy = width // n_y
    chunks = wy // wdev
    hidden = gate_weight.shape[1]
    experts = n_sp
    cap = 5 * tokens // (2 * experts)
    kx = cap // n_x
    slots = experts * kx
    padded = -(-cap // 8) * 8
    yi = lax.axis_index("y")
    xi = lax.axis_index("x")

    weights = jnp.concatenate([gate_weight, lin_weight, down_weight], axis=0)
    blocks = [weights] + [turned(weights, "x", d) for d in range(1, n_x)]

    send, place = route(
        route_ids, route_weights, moe_input, out_grad, yi, xi, n_y, kx, experts, cap, padded
    )
    got = swap(send.reshape(experts, kx * 2 * chunks, wdev), SP)
    (got,) = on_core(
        regroup_kernel, [((n_y, 2 * chunks, slots, wdev), BF)], got.reshape(slots, 2 * chunks, wdev)
    )
    got = swap(got, "y")

    part, cots = on_core(
        expert_kernel,
        [((n_tp, slots, wdev), BF), ((3, slots, n_x * hidden), BF)],
        got,
        *blocks,
        mib=24,
    )
    part = swap(part, TP)
    terms = on_core(weight_grad_kernel, [((3, hidden, width), BF)] * n_x, got, cots, mib=24)
    (slot_sums,) = on_core(
        slot_sum_kernel,
        [((experts * padded, wdev), BF)],
        part,
        n_y=n_y,
        n_x=n_x,
        kx=kx,
        padded=padded,
    )
    back = swap(slot_sums.reshape(experts, padded, wdev), SP)
    back = back.reshape(experts * padded, wdev)

    spread = [terms[0]] + [turned(terms[d], "x", -d) for d in range(1, n_x)]
    gate_grad, lin_grad, down_grad = (
        sum(t[k : k + 1].astype(F32) for t in spread).astype(BF) for k in range(3)
    )

    (row_grads,) = on_core(combine_kernel, [((n_tp, tokens, wdev), BF)], place.T, back)
    full = swap(row_grads, TP)

    taps = conv_taps.shape[0]
    conv_values = (inner_gate.astype(F32) * conv_input.astype(F32)).astype(BF)
    prior_rows = from_behind(conv_values[tokens - (taps - 1) :], SP, 1)
    extended = jnp.concatenate([prior_rows, conv_values], axis=0).astype(F32)
    convolved = jnp.zeros((tokens, wdev), F32)
    for tap in range(taps):
        convolved = convolved + conv_taps[tap][None, :] * extended[tap : tap + tokens]
    mixed = (outer_gate.astype(F32) * convolved).astype(BF)

    inner = 4
    proj = grouped(out_proj.T, "z", n_z // inner, inner)
    proj = grouped(proj, "z", inner, 1)
    twin = shifted(proj, "c", n_c, 1, 1)
    proj = with_twin(proj, twin, lax.axis_index("c")).reshape(width, wdev)
    pair, conv_cot, outer_gate_grad = mix(
        full, out_grad, proj, mixed, convolved, outer_gate, n_c, n_z
    )
    terms = swap(pair, "c")
    terms = jnp.sum(terms.astype(F32), axis=0).astype(BF)
    out_proj_grad = jnp.sum(swap(terms, "z").astype(F32), axis=0)

    later_rows = from_behind(conv_cot[: taps - 1], SP, -1)
    extended_cot = jnp.concatenate([conv_cot, later_rows], axis=0).astype(F32)
    value_grad = jnp.zeros((tokens, wdev), F32)
    for tap in range(taps):
        start = taps - 1 - tap
        value_grad = value_grad + conv_taps[tap][None, :] * extended_cot[start : start + tokens]
    inner_gate_grad = (value_grad * conv_input.astype(F32)).astype(BF)
    conv_input_grad = (value_grad * inner_gate.astype(F32)).astype(BF)
    return (
        gate_grad,
        lin_grad,
        down_grad,
        out_proj_grad,
        outer_gate_grad,
        inner_gate_grad,
        conv_input_grad,
    )


def solution(mesh):
    torus = Mesh(mesh.devices.reshape(-1, 2, 4, 4), ("z", "c", "y", "x"))
    tokens = P(SP, None)
    expert = P(SP, TP, None)
    mixer = P(SP, TP)
    return jax.shard_map(
        local,
        mesh=torus,
        in_specs=(tokens,) * 4 + (expert,) * 3 + (mixer,) * 3 + (P(None, TP), P(TP, SP)),
        out_specs=(expert,) * 3 + (mixer,) * 4,
        check_vma=False,
    )
```

```python
import functools

import jax
import jax.numpy as jnp
from jax import lax
from jax.experimental import pallas as pl
from jax.experimental.pallas import tpu as pltpu
from jax.sharding import Mesh
from jax.sharding import PartitionSpec as P


SP = ("z", "c")
TP = ("y", "x")
LIMIT = 7.0
ALPHA = 1.702
LANES = 128
BF = jnp.bfloat16
F32 = jnp.float32


def swap(blocks, axis):
    return lax.all_to_all(blocks, axis, split_axis=0, concat_axis=0, tiled=True)


def turned(value, axis, by):
    count = lax.axis_size(axis)
    return lax.ppermute(value, axis, [(i, (i + by) % count) for i in range(count)])


def shifted(value, axis, group, stride, by):
    count = lax.axis_size(axis)
    size = group * stride

    def source(i):
        return i // size * size + (i + by * stride) % size

    return lax.ppermute(value, axis, [(source(i), i) for i in range(count)])


def grouped(value, axis, group, stride):
    others = [shifted(value, axis, group, stride, by) for by in range(1, group)]
    place = lax.rem(lax.div(lax.axis_index(axis), jnp.int32(stride)), jnp.int32(group))
    return ordered([value, *others], place)


def from_behind(value, axis, by):
    count = lax.axis_size(axis)
    pairs = [(i, i + by) for i in range(count) if 0 <= i + by < count]
    return lax.ppermute(value, axis, pairs)


def dot(a, b, ca, cb):
    return lax.dot_general(a, b, (((ca,), (cb,)), ((), ())), preferred_element_type=F32)


def expert_cots(rows, grads, gate_w, lin_w, down_w):
    gate_pre = dot(rows, gate_w, 1, 1)
    lin_pre = dot(rows, lin_w, 1, 1)
    act_grad = dot(grads, down_w, 1, 1)
    gate_cut = jnp.minimum(gate_pre, LIMIT)
    lin_cut = jnp.clip(lin_pre, -LIMIT, LIMIT)
    sigma = jax.nn.sigmoid(ALPHA * gate_cut)
    act = (gate_cut * sigma * (lin_cut + 1.0)).astype(BF)
    slope = sigma * (1.0 + ALPHA * gate_cut * (1.0 - sigma))
    gate_cot = jnp.where(gate_pre < LIMIT, act_grad * (lin_cut + 1.0) * slope, 0.0).astype(BF)
    lin_cot = jnp.where(jnp.abs(lin_pre) < LIMIT, act_grad * gate_cut * sigma, 0.0).astype(BF)
    return act, gate_cot, lin_cot


def routing_kernel(yi_ref, xi_ref, core_ref, ids_ref, weights_ref, rows_ref, grads_ref, send_ref, place_ref, *, kx, cap):
    tokens = ids_ref.shape[1]
    experts = send_ref.shape[0] // kx
    ids = ids_ref[...]
    expert = lax.broadcasted_iota(jnp.int32, (experts, tokens), 0)
    first = expert == ids[0:1, :]
    second = expert == ids[1:2, :]
    one = jnp.where(first | second, 1.0, 0.0).astype(BF)
    early = lax.broadcasted_iota(jnp.int32, (tokens, tokens), 0)
    late = lax.broadcasted_iota(jnp.int32, (tokens, tokens), 1)
    before = dot(one, jnp.where(early < late, 1.0, 0.0).astype(BF), 1, 0)
    rank0 = jnp.sum(jnp.where(first, before, 0.0), axis=0, keepdims=True).astype(jnp.int32)
    rank1 = jnp.sum(jnp.where(second, before, 0.0), axis=0, keepdims=True).astype(jnp.int32)
    turn = jnp.where((ids & 1) == core_ref[0], 0, cap) - (ids & 1) * cap
    place_ref[0:1, :] = ids[0:1, :] * cap + turn[0:1, :] + rank0
    place_ref[1:2, :] = ids[1:2, :] * cap + turn[1:2, :] + rank1
    slots = experts * kx
    slot = lax.broadcasted_iota(jnp.int32, (slots, 1), 0)
    owner = slot // kx
    slot = owner * cap + xi_ref[0] * kx + (slot - owner * kx)
    hit0 = slot == ids[0:1, :] * cap + rank0
    hit1 = slot == ids[1:2, :] * cap + rank1
    pick = jnp.where(hit0 | hit1, 1.0, 0.0).astype(BF)
    w = weights_ref[...]
    weight = jnp.sum(
        jnp.where(hit0, w[0:1, :], 0.0) + jnp.where(hit1, w[1:2, :], 0.0), axis=1, keepdims=True
    )
    rows = dot(pick, rows_ref[...], 1, 0)
    grads = weight * dot(pick, grads_ref[...], 1, 0)
    both = jnp.concatenate([rows, grads], axis=1)
    send_ref[...] = both.reshape(slots, both.shape[1] // LANES, LANES).astype(BF)


def route(route_ids, route_weights, moe_input, out_grad, yi, xi, core, n_y, kx, experts, cap):
    tokens, width = moe_input.shape
    wy = width // n_y
    slots = experts * kx
    return pl.pallas_call(
        functools.partial(routing_kernel, kx=kx, cap=cap),
        grid_spec=pltpu.PrefetchScalarGridSpec(
            num_scalar_prefetch=3,
            grid=(1,),
            in_specs=[
                pl.BlockSpec((2, tokens), lambda i, y, x, c: (0, 0)),
                pl.BlockSpec((2, tokens), lambda i, y, x, c: (0, 0)),
                pl.BlockSpec((tokens, wy), lambda i, y, x, c: (0, y[0])),
                pl.BlockSpec((tokens, wy), lambda i, y, x, c: (0, y[0])),
            ],
            out_specs=[
                pl.BlockSpec((slots, 2 * wy // LANES, LANES), lambda i, y, x, c: (0, 0, 0)),
                pl.BlockSpec((2, tokens), lambda i, y, x, c: (0, 0)),
            ],
        ),
        out_shape=[
            jax.ShapeDtypeStruct((slots, 2 * wy // LANES, LANES), BF),
            jax.ShapeDtypeStruct((2, tokens), jnp.int32),
        ],
        name="route",
    )(yi[None], xi[None], core[None], route_ids.T, route_weights.T, moe_input, out_grad)


def regroup_kernel(got_ref, out_ref):
    _, both, _ = got_ref.shape
    got = got_ref[...].astype(F32)
    for f in range(both):
        piece = got[:, f, :].astype(BF)
        for y in range(out_ref.shape[0]):
            out_ref[y, f] = piece


def expert_kernel(got_ref, w0_ref, w1_ref, w2_ref, w3_ref, part_ref, cots_ref):
    n_y, both, _, lanes = got_ref.shape
    chunks = both // 2
    rows = jnp.concatenate([got_ref[y, f] for y in range(n_y) for f in range(chunks)], axis=1)
    grads = jnp.concatenate(
        [got_ref[y, chunks + f] for y in range(n_y) for f in range(chunks)], axis=1
    )
    refs = (w0_ref, w1_ref, w2_ref, w3_ref)
    gate_w, lin_w, down_w = (jnp.concatenate([r[k] for r in refs], axis=0) for k in range(3))
    act, gate_cot, lin_cot = expert_cots(rows, grads, gate_w, lin_w, down_w)
    cots_ref[0] = gate_cot
    cots_ref[1] = lin_cot
    cots_ref[2] = act
    part = dot(gate_cot, gate_w, 1, 0) + dot(lin_cot, lin_w, 1, 0)
    for t in range(part_ref.shape[0]):
        part_ref[t] = part[:, t * lanes : (t + 1) * lanes].astype(BF)


def weight_grad_kernel(got_ref, cots_ref, o0_ref, o1_ref, o2_ref, o3_ref):
    n_y, both, _, _ = got_ref.shape
    chunks = both // 2
    outs = (o0_ref, o1_ref, o2_ref, o3_ref)
    hidden = o0_ref.shape[1]
    for k in range(3):
        offset = chunks if k == 2 else 0
        other = jnp.concatenate(
            [got_ref[y, offset + f] for y in range(n_y) for f in range(chunks)], axis=1
        )
        terms = dot(cots_ref[k], other, 0, 0)
        for d, ref in enumerate(outs):
            ref[k] = terms[d * hidden : (d + 1) * hidden].astype(ref.dtype)


def slot_sum_kernel(core_ref, part_ref, keep_ref, give_ref, *, n_y, n_x, kx):
    _, slots, _ = part_ref.shape
    rows = keep_ref.shape[0]
    cap = n_x * kx
    row = lax.broadcasted_iota(jnp.int32, (rows, 1), 0)
    ring = row // cap
    at = row - ring * cap
    group = at // kx
    wanted = group * slots + 2 * ring * kx + (at - group * kx)
    col = lax.broadcasted_iota(jnp.int32, (rows, n_x * slots), 1)
    sums = []
    for x in range(n_x):
        total = part_ref[x].astype(F32)
        for y in range(1, n_y):
            total = total + part_ref[y * n_x + x].astype(F32)
        sums.append(total.astype(BF))
    sums = jnp.concatenate(sums, axis=0)
    for ref, core in ((keep_ref, core_ref[0]), (give_ref, 1 - core_ref[0])):
        pick = jnp.where(wanted + core * kx == col, 1.0, 0.0).astype(BF)
        ref[...] = dot(pick, sums, 1, 0).astype(BF)


def join_kernel(own_ref, other_ref, out_ref):
    rings, both, _ = out_ref.shape
    cap = both // 2
    own = own_ref[...].astype(F32)
    other = other_ref[...].astype(F32)
    for z in range(rings):
        at = slice(z * cap, (z + 1) * cap)
        out_ref[z] = jnp.concatenate([own[at], other[at]], axis=0).astype(BF)


def combine_kernel(place_ref, back_ref, out_ref):
    tokens = place_ref.shape[0]
    every = lax.broadcasted_iota(jnp.int32, (tokens, back_ref.shape[0]), 1)
    place = place_ref[...]
    hit = (every == place[:, 0:1]) | (every == place[:, 1:2])
    row_grads = dot(jnp.where(hit, 1.0, 0.0).astype(BF), back_ref[...], 1, 0).astype(BF)
    for t in range(out_ref.shape[0]):
        out_ref[t] = row_grads


def mixer_kernel(
    core_ref, full_ref, out_grad_ref, proj_ref, mixed_hbm, convolved_hbm, outer_hbm,
    keep_ref, give_ref, cot_ref, outer_grad_hbm,
    mixed_ref, convolved_ref, outer_ref, outer_grad_ref, sems,
):
    n_tp, _, _ = full_ref.shape
    n_z, per, _ = keep_ref.shape
    fetches = [
        pltpu.make_async_copy(src, dst, sems.at[i])
        for i, (src, dst) in enumerate(
            ((convolved_hbm, convolved_ref), (outer_hbm, outer_ref), (mixed_hbm, mixed_ref))
        )
    ]
    for fetch in fetches:
        fetch.start()
    full = jnp.concatenate([full_ref[t] for t in range(n_tp)], axis=1)
    stream = (out_grad_ref[...].astype(F32) + full.astype(F32)).astype(BF)
    mixed_grad = dot(stream, proj_ref[...], 1, 0)
    fetches[0].wait()
    outer_grad_ref[...] = (mixed_grad * convolved_ref[...]).astype(BF)
    keep = pltpu.make_async_copy(outer_grad_ref, outer_grad_hbm, sems.at[3])
    keep.start()
    fetches[1].wait()
    cot_ref[...] = (mixed_grad * outer_ref[...].astype(F32)).astype(BF)
    fetches[2].wait()
    terms = dot(stream, mixed_ref[...], 0, 0).astype(BF)
    lower = core_ref[0] == 0
    for z in range(n_z):
        low = terms[2 * z * per : (2 * z + 1) * per]
        high = terms[(2 * z + 1) * per : (2 * z + 2) * per]
        keep_ref[z] = jnp.where(lower, low, high)
        give_ref[z] = jnp.where(lower, high, low)
    keep.wait()


def order_kernel(place_ref, *refs):
    *parts, out_ref = refs
    for by, ref in enumerate(parts):
        at = place_ref[0] + by
        out_ref[jnp.where(at >= len(parts), at - len(parts), at)] = ref[...]


def ordered(parts, place):
    return pl.pallas_call(
        order_kernel,
        in_specs=[pl.BlockSpec(memory_space=pltpu.SMEM)]
        + [pl.BlockSpec(memory_space=pltpu.VMEM)] * len(parts),
        out_shape=jax.ShapeDtypeStruct((len(parts), *parts[0].shape), parts[0].dtype),
        compiler_params=pltpu.CompilerParams(vmem_limit_bytes=4 << 20),
    )(place[None], *parts)


def twin_kernel(place_ref, own_ref, other_ref, out_ref):
    near, far = own_ref.shape[:2]
    mine = place_ref[0]
    for f in range(far):
        for n in range(near):
            out_ref[f * near + n, mine] = own_ref[n, f]
            out_ref[f * near + n, 1 - mine] = other_ref[n, f]


def with_twin(own, other, place):
    near, far, *block = own.shape
    return pl.pallas_call(
        twin_kernel,
        in_specs=[pl.BlockSpec(memory_space=pltpu.SMEM)]
        + [pl.BlockSpec(memory_space=pltpu.VMEM)] * 2,
        out_shape=jax.ShapeDtypeStruct((far * near, 2, *block), own.dtype),
        compiler_params=pltpu.CompilerParams(vmem_limit_bytes=4 << 20),
        name="twins",
    )(place[None], own, other)


def in_hbm(value):
    return pltpu.with_memory_space_constraint(value, pltpu.HBM)


def mix(core, full, out_grad, proj, mixed, convolved, outer_gate, n_c, n_z):
    _, tokens, lanes = full.shape
    small = (tokens, lanes)
    whole = pl.BlockSpec(memory_space=pltpu.VMEM)
    away = pl.BlockSpec(memory_space=pltpu.HBM)
    half = (n_z, proj.shape[0] // (n_c * n_z), lanes)
    return pl.pallas_call(
        mixer_kernel,
        in_specs=[pl.BlockSpec(memory_space=pltpu.SMEM)] + [whole] * 3 + [away] * 3,
        out_specs=[whole, whole, whole, away],
        out_shape=[
            jax.ShapeDtypeStruct(half, BF),
            pltpu.HBM(half, BF),
            pltpu.HBM(small, BF),
            pltpu.HBM(small, BF),
        ],
        scratch_shapes=[
            pltpu.VMEM(small, BF),
            pltpu.VMEM(small, F32),
            pltpu.VMEM(small, BF),
            pltpu.VMEM(small, BF),
            pltpu.SemaphoreType.DMA((4,)),
        ],
        compiler_params=pltpu.CompilerParams(vmem_limit_bytes=16 << 20),
        name="mixer",
    )(core[None], full, out_grad, proj, *map(in_hbm, (mixed, convolved, outer_gate)))


def on_core(kernel, outs, *args, mib=12, scalars=0, **static):
    return pl.pallas_call(
        functools.partial(kernel, **static) if static else kernel,
        in_specs=[
            pl.BlockSpec(memory_space=pltpu.SMEM if i < scalars else pltpu.VMEM)
            for i in range(len(args))
        ],
        out_shape=[pltpu.HBM(s, t) for s, t in outs],
        compiler_params=pltpu.CompilerParams(vmem_limit_bytes=mib << 20),
    )(*args)


def local(
    moe_input,
    out_grad,
    route_ids,
    route_weights,
    gate_weight,
    lin_weight,
    down_weight,
    outer_gate,
    inner_gate,
    conv_input,
    conv_taps,
    out_proj,
):
    n_sp = lax.axis_size(SP)
    n_z, n_c, n_y, n_x = (lax.axis_size(a) for a in ("z", "c", "y", "x"))
    n_tp = n_y * n_x
    tokens, _ = route_ids.shape
    width = moe_input.shape[1]
    wdev = width // n_tp
    wy = width // n_y
    chunks = wy // wdev
    hidden = gate_weight.shape[1]
    experts = n_sp
    cap = 5 * tokens // (2 * experts)
    kx = cap // n_x
    slots = experts * kx
    yi = lax.axis_index("y")
    xi = lax.axis_index("x")

    weights = jnp.concatenate([gate_weight, lin_weight, down_weight], axis=0)
    blocks = [weights] + [turned(weights, "x", d) for d in range(1, n_x)]

    core = lax.axis_index("c")
    send, place = route(
        route_ids, route_weights, moe_input, out_grad, yi, xi, core, n_y, kx, experts, cap
    )
    got = swap(send.reshape(experts, kx * 2 * chunks, wdev), SP)
    (got,) = on_core(
        regroup_kernel, [((n_y, 2 * chunks, slots, wdev), BF)], got.reshape(slots, 2 * chunks, wdev)
    )
    got = swap(got, "y")

    part, cots = on_core(
        expert_kernel,
        [((n_tp, slots, wdev), BF), ((3, slots, n_x * hidden), BF)],
        got,
        *blocks,
        mib=24,
    )
    part = swap(part, TP)
    terms = on_core(weight_grad_kernel, [((3, hidden, width), BF)] * n_x, got, cots, mib=24)
    held, given = on_core(
        slot_sum_kernel,
        [((n_z * cap, wdev), BF)] * 2,
        core[None],
        part,
        n_y=n_y,
        n_x=n_x,
        kx=kx,
        scalars=1,
    )
    given = shifted(given, "c", n_c, 1, 1)
    (joined,) = on_core(join_kernel, [((n_z, 2 * cap, wdev), BF)], held, given)
    back = swap(joined, "z").reshape(experts * cap, wdev)

    spread = [terms[0]] + [turned(terms[d], "x", -d) for d in range(1, n_x)]
    gate_grad, lin_grad, down_grad = (
        sum(t[k : k + 1].astype(F32) for t in spread).astype(BF) for k in range(3)
    )

    (row_grads,) = on_core(combine_kernel, [((n_tp, tokens, wdev), BF)], place.T, back)
    full = swap(row_grads, TP)

    taps = conv_taps.shape[0]
    conv_values = (inner_gate.astype(F32) * conv_input.astype(F32)).astype(BF)
    prior_rows = from_behind(conv_values[tokens - (taps - 1) :], SP, 1)
    extended = jnp.concatenate([prior_rows, conv_values], axis=0).astype(F32)
    convolved = jnp.zeros((tokens, wdev), F32)
    for tap in range(taps):
        convolved = convolved + conv_taps[tap][None, :] * extended[tap : tap + tokens]
    mixed = (outer_gate.astype(F32) * convolved).astype(BF)

    inner = 4
    proj = grouped(out_proj.T, "z", n_z // inner, inner)
    proj = grouped(proj, "z", inner, 1)
    twin = shifted(proj, "c", n_c, 1, 1)
    proj = with_twin(proj, twin, core).reshape(width, wdev)
    keep, give, conv_cot, outer_gate_grad = mix(
        core, full, out_grad, proj, mixed, convolved, outer_gate, n_c, n_z
    )
    given = shifted(give, "c", n_c, 1, 1)
    terms = (keep.astype(F32) + given.astype(F32)).astype(BF)
    out_proj_grad = jnp.sum(swap(terms, "z").astype(F32), axis=0)

    later_rows = from_behind(conv_cot[: taps - 1], SP, -1)
    extended_cot = jnp.concatenate([conv_cot, later_rows], axis=0).astype(F32)
    value_grad = jnp.zeros((tokens, wdev), F32)
    for tap in range(taps):
        start = taps - 1 - tap
        value_grad = value_grad + conv_taps[tap][None, :] * extended_cot[start : start + tokens]
    inner_gate_grad = (value_grad * conv_input.astype(F32)).astype(BF)
    conv_input_grad = (value_grad * inner_gate.astype(F32)).astype(BF)
    return (
        gate_grad,
        lin_grad,
        down_grad,
        out_proj_grad,
        outer_gate_grad,
        inner_gate_grad,
        conv_input_grad,
    )


def solution(mesh):
    torus = Mesh(mesh.devices.reshape(-1, 2, 4, 4), ("z", "c", "y", "x"))
    tokens = P(SP, None)
    expert = P(SP, TP, None)
    mixer = P(SP, TP)
    return jax.shard_map(
        local,
        mesh=torus,
        in_specs=(tokens,) * 4 + (expert,) * 3 + (mixer,) * 3 + (P(None, TP), P(TP, SP)),
        out_specs=(expert,) * 3 + (mixer,) * 4,
        check_vma=False,
    )
```

```python
import functools

import jax
import jax.numpy as jnp
from jax import lax
from jax.experimental import pallas as pl
from jax.experimental.pallas import tpu as pltpu
from jax.sharding import Mesh
from jax.sharding import PartitionSpec as P


SP = ("z", "c")
TP = ("y", "x")
LIMIT = 7.0
ALPHA = 1.702
LANES = 128
BF = jnp.bfloat16
F32 = jnp.float32


def swap(blocks, axis):
    return lax.all_to_all(blocks, axis, split_axis=0, concat_axis=0, tiled=True)


def turned(value, axis, by):
    count = lax.axis_size(axis)
    return lax.ppermute(value, axis, [(i, (i + by) % count) for i in range(count)])


def shifted(value, axis, group, stride, by):
    count = lax.axis_size(axis)
    size = group * stride

    def source(i):
        return i // size * size + (i + by * stride) % size

    return lax.ppermute(value, axis, [(source(i), i) for i in range(count)])


def grouped(value, axis, group, stride):
    others = [shifted(value, axis, group, stride, by) for by in range(1, group)]
    place = lax.rem(lax.div(lax.axis_index(axis), jnp.int32(stride)), jnp.int32(group))
    return ordered([value, *others], place)


def from_behind(value, axis, by):
    count = lax.axis_size(axis)
    pairs = [(i, i + by) for i in range(count) if 0 <= i + by < count]
    return lax.ppermute(value, axis, pairs)


def dot(a, b, ca, cb):
    return lax.dot_general(a, b, (((ca,), (cb,)), ((), ())), preferred_element_type=F32)


def expert_cots(rows, grads, gate_w, lin_w, down_w):
    gate_pre = dot(rows, gate_w, 1, 1)
    lin_pre = dot(rows, lin_w, 1, 1)
    act_grad = dot(grads, down_w, 1, 1)
    gate_cut = jnp.minimum(gate_pre, LIMIT)
    lin_cut = jnp.clip(lin_pre, -LIMIT, LIMIT)
    sigma = jax.nn.sigmoid(ALPHA * gate_cut)
    act = (gate_cut * sigma * (lin_cut + 1.0)).astype(BF)
    slope = sigma * (1.0 + ALPHA * gate_cut * (1.0 - sigma))
    gate_cot = jnp.where(gate_pre < LIMIT, act_grad * (lin_cut + 1.0) * slope, 0.0).astype(BF)
    lin_cot = jnp.where(jnp.abs(lin_pre) < LIMIT, act_grad * gate_cut * sigma, 0.0).astype(BF)
    return act, gate_cot, lin_cot


def routing_kernel(yi_ref, xi_ref, ids_ref, weights_ref, rows_ref, grads_ref, send_ref, place_ref, *, kx, cap, padded):
    tokens = ids_ref.shape[1]
    experts = send_ref.shape[0] // kx
    ids = ids_ref[...]
    expert = lax.broadcasted_iota(jnp.int32, (experts, tokens), 0)
    first = expert == ids[0:1, :]
    second = expert == ids[1:2, :]
    one = jnp.where(first | second, 1.0, 0.0).astype(BF)
    early = lax.broadcasted_iota(jnp.int32, (tokens, tokens), 0)
    late = lax.broadcasted_iota(jnp.int32, (tokens, tokens), 1)
    before = dot(one, jnp.where(early < late, 1.0, 0.0).astype(BF), 1, 0)
    rank0 = jnp.sum(jnp.where(first, before, 0.0), axis=0, keepdims=True).astype(jnp.int32)
    rank1 = jnp.sum(jnp.where(second, before, 0.0), axis=0, keepdims=True).astype(jnp.int32)
    place_ref[0:1, :] = ids[0:1, :] * padded + rank0
    place_ref[1:2, :] = ids[1:2, :] * padded + rank1
    slots = experts * kx
    slot = lax.broadcasted_iota(jnp.int32, (slots, 1), 0)
    owner = slot // kx
    slot = owner * cap + xi_ref[0] * kx + (slot - owner * kx)
    hit0 = slot == ids[0:1, :] * cap + rank0
    hit1 = slot == ids[1:2, :] * cap + rank1
    pick = jnp.where(hit0 | hit1, 1.0, 0.0).astype(BF)
    w = weights_ref[...]
    weight = jnp.sum(
        jnp.where(hit0, w[0:1, :], 0.0) + jnp.where(hit1, w[1:2, :], 0.0), axis=1, keepdims=True
    )
    rows = dot(pick, rows_ref[...], 1, 0)
    grads = weight * dot(pick, grads_ref[...], 1, 0)
    both = jnp.concatenate([rows, grads], axis=1)
    send_ref[...] = both.reshape(slots, both.shape[1] // LANES, LANES).astype(BF)


def route(route_ids, route_weights, moe_input, out_grad, yi, xi, n_y, kx, experts, cap, padded):
    tokens, width = moe_input.shape
    wy = width // n_y
    slots = experts * kx
    return pl.pallas_call(
        functools.partial(routing_kernel, kx=kx, cap=cap, padded=padded),
        grid_spec=pltpu.PrefetchScalarGridSpec(
            num_scalar_prefetch=2,
            grid=(1,),
            in_specs=[
                pl.BlockSpec((2, tokens), lambda i, y, x: (0, 0)),
                pl.BlockSpec((2, tokens), lambda i, y, x: (0, 0)),
                pl.BlockSpec((tokens, wy), lambda i, y, x: (0, y[0])),
                pl.BlockSpec((tokens, wy), lambda i, y, x: (0, y[0])),
            ],
            out_specs=[
                pl.BlockSpec((slots, 2 * wy // LANES, LANES), lambda i, y, x: (0, 0, 0)),
                pl.BlockSpec((2, tokens), lambda i, y, x: (0, 0)),
            ],
        ),
        out_shape=[
            jax.ShapeDtypeStruct((slots, 2 * wy // LANES, LANES), BF),
            jax.ShapeDtypeStruct((2, tokens), jnp.int32),
        ],
        name="route",
    )(yi[None], xi[None], route_ids.T, route_weights.T, moe_input, out_grad)


def regroup_kernel(got_ref, out_ref):
    _, both, _ = got_ref.shape
    got = got_ref[...].astype(F32)
    for f in range(both):
        piece = got[:, f, :].astype(BF)
        for y in range(out_ref.shape[0]):
            out_ref[y, f] = piece


def expert_kernel(got_ref, w0_ref, w1_ref, w2_ref, w3_ref, part_ref, cots_ref):
    n_y, both, _, lanes = got_ref.shape
    chunks = both // 2
    rows = jnp.concatenate([got_ref[y, f] for y in range(n_y) for f in range(chunks)], axis=1)
    grads = jnp.concatenate(
        [got_ref[y, chunks + f] for y in range(n_y) for f in range(chunks)], axis=1
    )
    refs = (w0_ref, w1_ref, w2_ref, w3_ref)
    gate_w, lin_w, down_w = (jnp.concatenate([r[k] for r in refs], axis=0) for k in range(3))
    act, gate_cot, lin_cot = expert_cots(rows, grads, gate_w, lin_w, down_w)
    cots_ref[0] = gate_cot
    cots_ref[1] = lin_cot
    cots_ref[2] = act
    part = dot(gate_cot, gate_w, 1, 0) + dot(lin_cot, lin_w, 1, 0)
    for t in range(part_ref.shape[0]):
        part_ref[t] = part[:, t * lanes : (t + 1) * lanes].astype(BF)


def weight_grad_kernel(got_ref, cots_ref, o0_ref, o1_ref, o2_ref, o3_ref):
    n_y, both, _, _ = got_ref.shape
    chunks = both // 2
    outs = (o0_ref, o1_ref, o2_ref, o3_ref)
    hidden = o0_ref.shape[1]
    for k in range(3):
        offset = chunks if k == 2 else 0
        other = jnp.concatenate(
            [got_ref[y, offset + f] for y in range(n_y) for f in range(chunks)], axis=1
        )
        terms = dot(cots_ref[k], other, 0, 0)
        for d, ref in enumerate(outs):
            ref[k] = terms[d * hidden : (d + 1) * hidden].astype(ref.dtype)


def slot_sum_kernel(part_ref, out_ref, *, n_y, n_x, kx, padded):
    _, slots, _ = part_ref.shape
    rows = out_ref.shape[0]
    cols = n_x * slots
    row = lax.broadcasted_iota(jnp.int32, (rows, 1), 0)
    owner = row // padded
    at = row - owner * padded
    group = at // kx
    wanted = jnp.where(group < n_x, group * slots + owner * kx + (at - group * kx), -1)
    col = lax.broadcasted_iota(jnp.int32, (rows, cols), 1)
    pick = jnp.where(wanted == col, 1.0, 0.0).astype(BF)
    sums = []
    for x in range(n_x):
        total = part_ref[x].astype(F32)
        for y in range(1, n_y):
            total = total + part_ref[y * n_x + x].astype(F32)
        sums.append(total.astype(BF))
    out_ref[...] = dot(pick, jnp.concatenate(sums, axis=0), 1, 0).astype(BF)


def combine_kernel(place_ref, back_ref, out_ref):
    tokens = place_ref.shape[0]
    every = lax.broadcasted_iota(jnp.int32, (tokens, back_ref.shape[0]), 1)
    place = place_ref[...]
    hit = (every == place[:, 0:1]) | (every == place[:, 1:2])
    row_grads = dot(jnp.where(hit, 1.0, 0.0).astype(BF), back_ref[...], 1, 0).astype(BF)
    for t in range(out_ref.shape[0]):
        out_ref[t] = row_grads


def mixer_kernel(
    core_ref, full_ref, out_grad_ref, proj_ref, mixed_hbm, convolved_hbm, outer_hbm,
    keep_ref, give_ref, cot_ref, outer_grad_hbm,
    mixed_ref, convolved_ref, outer_ref, outer_grad_ref, sems,
):
    n_tp, _, _ = full_ref.shape
    n_z, per, _ = keep_ref.shape
    fetches = [
        pltpu.make_async_copy(src, dst, sems.at[i])
        for i, (src, dst) in enumerate(
            ((convolved_hbm, convolved_ref), (outer_hbm, outer_ref), (mixed_hbm, mixed_ref))
        )
    ]
    for fetch in fetches:
        fetch.start()
    full = jnp.concatenate([full_ref[t] for t in range(n_tp)], axis=1)
    stream = (out_grad_ref[...].astype(F32) + full.astype(F32)).astype(BF)
    mixed_grad = dot(stream, proj_ref[...], 1, 0)
    fetches[0].wait()
    outer_grad_ref[...] = (mixed_grad * convolved_ref[...]).astype(BF)
    keep = pltpu.make_async_copy(outer_grad_ref, outer_grad_hbm, sems.at[3])
    keep.start()
    fetches[1].wait()
    cot_ref[...] = (mixed_grad * outer_ref[...].astype(F32)).astype(BF)
    fetches[2].wait()
    terms = dot(stream, mixed_ref[...], 0, 0).astype(BF)
    lower = core_ref[0] == 0
    for z in range(n_z):
        low = terms[2 * z * per : (2 * z + 1) * per]
        high = terms[(2 * z + 1) * per : (2 * z + 2) * per]
        keep_ref[z] = jnp.where(lower, low, high)
        give_ref[z] = jnp.where(lower, high, low)
    keep.wait()


def order_kernel(place_ref, *refs):
    *parts, out_ref = refs
    for by, ref in enumerate(parts):
        at = place_ref[0] + by
        out_ref[jnp.where(at >= len(parts), at - len(parts), at)] = ref[...]


def ordered(parts, place):
    return pl.pallas_call(
        order_kernel,
        in_specs=[pl.BlockSpec(memory_space=pltpu.SMEM)]
        + [pl.BlockSpec(memory_space=pltpu.VMEM)] * len(parts),
        out_shape=jax.ShapeDtypeStruct((len(parts), *parts[0].shape), parts[0].dtype),
        compiler_params=pltpu.CompilerParams(vmem_limit_bytes=4 << 20),
    )(place[None], *parts)


def twin_kernel(place_ref, own_ref, other_ref, out_ref):
    near, far = own_ref.shape[:2]
    mine = place_ref[0]
    for f in range(far):
        for n in range(near):
            out_ref[f * near + n, mine] = own_ref[n, f]
            out_ref[f * near + n, 1 - mine] = other_ref[n, f]


def with_twin(own, other, place):
    near, far, *block = own.shape
    return pl.pallas_call(
        twin_kernel,
        in_specs=[pl.BlockSpec(memory_space=pltpu.SMEM)]
        + [pl.BlockSpec(memory_space=pltpu.VMEM)] * 2,
        out_shape=jax.ShapeDtypeStruct((far * near, 2, *block), own.dtype),
        compiler_params=pltpu.CompilerParams(vmem_limit_bytes=4 << 20),
        name="twins",
    )(place[None], own, other)


def in_hbm(value):
    return pltpu.with_memory_space_constraint(value, pltpu.HBM)


def mix(core, full, out_grad, proj, mixed, convolved, outer_gate, n_c, n_z):
    _, tokens, lanes = full.shape
    small = (tokens, lanes)
    whole = pl.BlockSpec(memory_space=pltpu.VMEM)
    away = pl.BlockSpec(memory_space=pltpu.HBM)
    half = (n_z, proj.shape[0] // (n_c * n_z), lanes)
    return pl.pallas_call(
        mixer_kernel,
        in_specs=[pl.BlockSpec(memory_space=pltpu.SMEM)] + [whole] * 3 + [away] * 3,
        out_specs=[whole, whole, whole, away],
        out_shape=[
            jax.ShapeDtypeStruct(half, BF),
            pltpu.HBM(half, BF),
            pltpu.HBM(small, BF),
            pltpu.HBM(small, BF),
        ],
        scratch_shapes=[
            pltpu.VMEM(small, BF),
            pltpu.VMEM(small, F32),
            pltpu.VMEM(small, BF),
            pltpu.VMEM(small, BF),
            pltpu.SemaphoreType.DMA((4,)),
        ],
        compiler_params=pltpu.CompilerParams(vmem_limit_bytes=16 << 20),
        name="mixer",
    )(core[None], full, out_grad, proj, *map(in_hbm, (mixed, convolved, outer_gate)))


def on_core(kernel, outs, *args, mib=12, **static):
    return pl.pallas_call(
        functools.partial(kernel, **static) if static else kernel,
        out_shape=[pltpu.HBM(s, t) for s, t in outs],
        compiler_params=pltpu.CompilerParams(vmem_limit_bytes=mib << 20),
    )(*args)


def local(
    moe_input,
    out_grad,
    route_ids,
    route_weights,
    gate_weight,
    lin_weight,
    down_weight,
    outer_gate,
    inner_gate,
    conv_input,
    conv_taps,
    out_proj,
):
    n_sp = lax.axis_size(SP)
    n_z, n_c, n_y, n_x = (lax.axis_size(a) for a in ("z", "c", "y", "x"))
    n_tp = n_y * n_x
    tokens, _ = route_ids.shape
    width = moe_input.shape[1]
    wdev = width // n_tp
    wy = width // n_y
    chunks = wy // wdev
    hidden = gate_weight.shape[1]
    experts = n_sp
    cap = 5 * tokens // (2 * experts)
    kx = cap // n_x
    slots = experts * kx
    padded = -(-cap // 8) * 8
    yi = lax.axis_index("y")
    xi = lax.axis_index("x")

    weights = jnp.concatenate([gate_weight, lin_weight, down_weight], axis=0)
    blocks = [weights] + [turned(weights, "x", d) for d in range(1, n_x)]

    send, place = route(
        route_ids, route_weights, moe_input, out_grad, yi, xi, n_y, kx, experts, cap, padded
    )
    got = swap(send.reshape(experts, kx * 2 * chunks, wdev), SP)
    (got,) = on_core(
        regroup_kernel, [((n_y, 2 * chunks, slots, wdev), BF)], got.reshape(slots, 2 * chunks, wdev)
    )
    got = swap(got, "y")

    part, cots = on_core(
        expert_kernel,
        [((n_tp, slots, wdev), BF), ((3, slots, n_x * hidden), BF)],
        got,
        *blocks,
        mib=24,
    )
    part = swap(part, TP)
    terms = on_core(weight_grad_kernel, [((3, hidden, width), BF)] * n_x, got, cots, mib=24)
    (slot_sums,) = on_core(
        slot_sum_kernel,
        [((experts * padded, wdev), BF)],
        part,
        n_y=n_y,
        n_x=n_x,
        kx=kx,
        padded=padded,
    )
    back = swap(slot_sums.reshape(experts, padded, wdev), SP)
    back = back.reshape(experts * padded, wdev)

    spread = [terms[0]] + [turned(terms[d], "x", -d) for d in range(1, n_x)]
    gate_grad, lin_grad, down_grad = (
        sum(t[k : k + 1].astype(F32) for t in spread).astype(BF) for k in range(3)
    )

    (row_grads,) = on_core(combine_kernel, [((n_tp, tokens, wdev), BF)], place.T, back)
    full = swap(row_grads, TP)

    taps = conv_taps.shape[0]
    conv_values = (inner_gate.astype(F32) * conv_input.astype(F32)).astype(BF)
    prior_rows = from_behind(conv_values[tokens - (taps - 1) :], SP, 1)
    extended = jnp.concatenate([prior_rows, conv_values], axis=0).astype(F32)
    convolved = jnp.zeros((tokens, wdev), F32)
    for tap in range(taps):
        convolved = convolved + conv_taps[tap][None, :] * extended[tap : tap + tokens]
    mixed = (outer_gate.astype(F32) * convolved).astype(BF)

    inner = 4
    proj = grouped(out_proj.T, "z", n_z // inner, inner)
    proj = grouped(proj, "z", inner, 1)
    twin = shifted(proj, "c", n_c, 1, 1)
    core = lax.axis_index("c")
    proj = with_twin(proj, twin, core).reshape(width, wdev)
    keep, give, conv_cot, outer_gate_grad = mix(
        core, full, out_grad, proj, mixed, convolved, outer_gate, n_c, n_z
    )
    given = shifted(give, "c", n_c, 1, 1)
    terms = (keep.astype(F32) + given.astype(F32)).astype(BF)
    out_proj_grad = jnp.sum(swap(terms, "z").astype(F32), axis=0)

    later_rows = from_behind(conv_cot[: taps - 1], SP, -1)
    extended_cot = jnp.concatenate([conv_cot, later_rows], axis=0).astype(F32)
    value_grad = jnp.zeros((tokens, wdev), F32)
    for tap in range(taps):
        start = taps - 1 - tap
        value_grad = value_grad + conv_taps[tap][None, :] * extended_cot[start : start + tokens]
    inner_gate_grad = (value_grad * conv_input.astype(F32)).astype(BF)
    conv_input_grad = (value_grad * inner_gate.astype(F32)).astype(BF)
    return (
        gate_grad,
        lin_grad,
        down_grad,
        out_proj_grad,
        outer_gate_grad,
        inner_gate_grad,
        conv_input_grad,
    )


def solution(mesh):
    torus = Mesh(mesh.devices.reshape(-1, 2, 4, 4), ("z", "c", "y", "x"))
    tokens = P(SP, None)
    expert = P(SP, TP, None)
    mixer = P(SP, TP)
    return jax.shard_map(
        local,
        mesh=torus,
        in_specs=(tokens,) * 4 + (expert,) * 3 + (mixer,) * 3 + (P(None, TP), P(TP, SP)),
        out_specs=(expert,) * 3 + (mixer,) * 4,
        check_vma=False,
    )
```
